32 devices in a mesh: rep: 2 (over x), fs: 4 (over z), tp: 4 (over y, core).
Axes of the slice: x: 2, y: 2, z: 4, core: 2. Of those that a mesh axis runs over, the one named last changes fastest.
Arguments:
- tokens: bfloat16 [4096, 2048], P(('rep', 'fs', 'tp')), may hold values from -6 to 6
- norm1_gain: float32 [2048], replicated, may hold values from 0.1 to 1.9
- in_weight: bfloat16 [2048, 1024], P('fs', 'tp'), may hold values from -0.125 to 0.125
- group_weight: bfloat16 [8, 128, 128], P('tp'), may hold values from -0.5 to 0.5
- pool_scale: float32 [1024], P('tp'), may hold values from 0.1 to 1.9
- out_weight: bfloat16 [1024, 2048], P('tp', 'fs'), may hold values from -0.1875 to 0.1875
- norm2_gain: float32 [2048], replicated, may hold values from 0.1 to 1.9
- up_weight: bfloat16 [2048, 8192], P('fs', 'tp'), may hold values from -0.125 to 0.125
- down_weight: bfloat16 [8192, 2048], P('tp', 'fs'), may hold values from -0.0625 to 0.0625
Outputs:
- layer_out: bfloat16 [4096, 2048], P(('rep', 'fs', 'tp'))
The draws below stay inside these ranges and needn't reach their ends.
All inputs are finite; a program needn't handle non-finite values.
Results may differ from the reference program's by a relative error of at most 0.02.
Values may be sent and summed in bfloat16 or wider, within the bound.
A program may use at most 128 MiB of HBM per device.

```python
import jax
import jax.numpy as jnp
from jax import lax

D = 2048
GROUPS = 8
GROUP_DIM = 128
FF = 8192
POOL = 1024
SEQ = 512
TOKENS = 4096
N_TP = 4


def block_levels(own_key, dims, shards, smallest, largest):
    def one(dim, blocks):
        steps = jax.random.uniform(jax.random.fold_in(jax.random.fold_in(own_key, 6), dim), (blocks,), jnp.float32, smallest / len(shards), largest / len(shards))
        return jnp.repeat(jnp.exp(steps), dims[dim] // blocks).reshape((-1,) + (1,) * (len(dims) - dim - 1))

    loudness = one(*shards[0])
    for cut in shards[1:]:
        loudness = loudness * one(*cut)
    return loudness


def normal_values(rng, shape, scale, most, cuts=(), kind=jnp.bfloat16):
    values = scale * jax.random.normal(rng, shape, jnp.float32)
    if cuts:
        values = values * block_levels(rng, shape, cuts, -0.22, 0.18)
    return jnp.clip(values, -most, most).astype(kind)


def setup_inputs(seed: int = 0) -> dict:
    streams_of = jax.random.split(jax.random.key(seed), 10)
    return {
        "tokens": normal_values(streams_of[0], (TOKENS, D), 1.0, 6.0, ((0, 32),)),
        "norm1_gain": jnp.clip(1.0 + 0.18 * jax.random.normal(streams_of[1], (D,), jnp.float32), 0.1, 1.9),
        "in_weight": normal_values(streams_of[2], (D, POOL), D ** -0.5, 0.125, ((0, 4), (1, 4))),
        "group_weight": normal_values(streams_of[3], (GROUPS, GROUP_DIM, GROUP_DIM), GROUP_DIM ** -0.5, 0.5, ((0, 4),)),
        "pool_scale": jnp.clip(1.0 + 0.18 * jax.random.normal(streams_of[4], (POOL,), jnp.float32), 0.1, 1.9),
        "out_weight": normal_values(streams_of[5], (POOL, D), POOL ** -0.5, 0.1875, ((0, 4), (1, 4))),
        "norm2_gain": jnp.clip(1.0 + 0.18 * jax.random.normal(streams_of[6], (D,), jnp.float32), 0.1, 1.9),
        "up_weight": normal_values(streams_of[7], (D, FF), D ** -0.5, 0.125, ((0, 4), (1, 4))),
        "down_weight": normal_values(streams_of[8], (FF, D), FF ** -0.5, 0.0625, ((0, 4), (1, 4))),
    }


epsilon = 1e-06

def rms_norm(values, gain):
    scale = lax.rsqrt(lax.optimization_barrier(jnp.mean(values * values, axis=-1, keepdims=True)) + epsilon)
    return values * scale * gain

def one_sequence(rows, norm1_gain, in_weight, group_weight, pool_scale, out_weight, norm2_gain, up_weight, down_weight):
    stream = rows.astype(jnp.float32)
    normed = rms_norm(stream, norm1_gain).astype(jnp.bfloat16)
    projected = jnp.dot(normed, in_weight, preferred_element_type=jnp.float32).astype(jnp.bfloat16)
    values = projected.astype(jnp.float32).reshape(SEQ, GROUPS, GROUP_DIM)
    totals = jnp.cumsum(values, axis=0)
    padded = jnp.pad(totals, ((16, 0), (0, 0), (0, 0)))
    position = jnp.arange(SEQ, dtype=jnp.int32)[:, None, None]
    group_level = (jnp.arange(GROUPS, dtype=jnp.int32) % 4)[None, :, None]
    window_mean = jnp.zeros((SEQ, GROUPS, GROUP_DIM), jnp.float32)
    for level in range(4):
        width = 2 ** (level + 1)
        sums = totals - padded[16 - width:16 - width + SEQ]
        count = jnp.minimum(position + 1, width).astype(jnp.float32)
        window_mean = jnp.where(group_level == level, sums / count, window_mean)
    pooled = (window_mean - values).astype(jnp.bfloat16)
    mapped = jnp.einsum('sgc,gcd->sgd', pooled.astype(jnp.float32), group_weight.astype(jnp.float32))
    pool_out = (mapped.reshape(SEQ, POOL) * pool_scale).astype(jnp.bfloat16)
    mixed_stream = stream + jnp.dot(pool_out, out_weight, preferred_element_type=jnp.float32)
    normed_two = rms_norm(mixed_stream, norm2_gain).astype(jnp.bfloat16)
    upper = jnp.dot(normed_two, up_weight, preferred_element_type=jnp.float32)
    hidden = jnp.square(jax.nn.relu(upper)).astype(jnp.bfloat16)
    block = FF // N_TP
    channel_sum = jnp.zeros((SEQ, D), jnp.float32)
    for index in range(N_TP):
        partial_sum = jnp.dot(hidden[:, index * block:(index + 1) * block], down_weight[index * block:(index + 1) * block], preferred_element_type=jnp.float32).astype(jnp.bfloat16)
        channel_sum = channel_sum + lax.optimization_barrier(partial_sum).astype(jnp.float32)
    return (mixed_stream + channel_sum).astype(jnp.bfloat16)

def reference(tokens, norm1_gain, in_weight, group_weight, pool_scale, out_weight, norm2_gain, up_weight, down_weight):
    sequences = tokens.reshape(TOKENS // SEQ, SEQ, D)

    def apply(rows):
        return one_sequence(rows, norm1_gain, in_weight, group_weight, pool_scale, out_weight, norm2_gain, up_weight, down_weight)
    return lax.map(apply, sequences).reshape(TOKENS, D)
```

```python
import functools

import jax
import jax.numpy as jnp
from jax import lax
from jax.experimental import pallas as pl
from jax.experimental.pallas import tpu as pltpu
from jax.sharding import PartitionSpec as P

MESH = pl.DeviceIdType.MESH
CHUNK_BYTES = 128 * 1024
SUB_COLUMNS = 256
LEVELS = 4

epsilon = 1e-06


def chunks_of(rows, columns, parts):
    count = max(1, rows * columns * 2 // parts // CHUNK_BYTES)
    while (rows // parts) % (count * 16):
        count -= 1
    return count


def dot(a, b):
    return jnp.dot(a, b, preferred_element_type=jnp.float32)


def tile_of(columns, most):
    tile = min(columns, most)
    while columns % tile:
        tile //= 2
    return tile


def kernel(
    sizes,
    tokens,
    gain1,
    in_hbm,
    group_weight,
    pool_scale,
    out_hbm,
    gain2,
    up_hbm,
    down_hbm,
    result,
    in_buf,
    out_buf,
    up_buf,
    down_buf,
    up_stage,
    down_stage,
    normed,
    projected,
    pool_out,
    mix_send,
    mix_recv,
    stream2,
    shared,
    hidden,
    core_send,
    core_recv,
    line_send,
    line_recv,
    pair_send,
    pair_recv,
    local_sem,
    in_sems,
    out_sems,
    up_sems,
    down_sems,
    tp_send,
    tp_recv,
    share_send,
    share_recv,
    core_sems,
    line_sems,
    pair_sems,
):
    n_rep, n_fs, n_tp = sizes
    n_y = n_tp // 2
    r, f, t = lax.axis_index("rep"), lax.axis_index("fs"), lax.axis_index("tp")
    core, y = lax.rem(t, 2), t // 2
    half = lax.rem(f, 2)
    f_pair, t_pair = f + 1 - 2 * half, t + 1 - 2 * core
    rows = tokens.shape[0]
    length = rows * n_tp
    width = tokens.shape[1]
    part = width // n_fs
    subs = down_buf.shape[1]
    sub_columns = down_buf.shape[3]
    steps = n_fs * subs
    half_units = up_buf.shape[3]
    gathered = ((in_buf, in_sems), (out_buf, out_sems))
    chunk_counts = [chunks_of(b.shape[1], b.shape[2], n_rep) for b, _ in gathered]
    spread = ((up_buf, up_stage, up_sems), (down_buf, down_stage, down_sems))
    spread_counts = [chunks_of(b.shape[2], b.shape[3], n_rep) for b, _, _ in spread]

    loads = []

    def load(source, target):
        copy = pltpu.make_async_copy(source, target, local_sem.at[len(loads)])
        copy.start()
        loads.append(copy)

    def units_of(which):
        return pl.ds(pl.multiple_of(which * half_units, half_units), half_units)

    load(in_hbm, in_buf.at[f])
    load(out_hbm, out_buf.at[f])
    load(up_hbm.at[:, units_of(1 - half)], up_stage.at[0])
    load(up_hbm.at[:, units_of(half)], up_buf.at[f, 0])
    for s in range(subs):
        columns = pl.ds(s * sub_columns, sub_columns)
        load(down_hbm.at[units_of(1 - half), columns], down_stage.at[s])
        load(down_hbm.at[units_of(half), columns], down_buf.at[f, s])

    barrier = pltpu.get_barrier_semaphore()
    greeted = [{"fs": lax.rem(f + d, n_fs)} for d in range(1, n_fs)]
    greeted += [{"rep": lax.rem(r + d, n_rep)} for d in range(1, n_rep)]
    greeted += [{"tp": lax.rem(t + d, n_tp)} for d in range(1, n_tp)]
    for device in greeted:
        pl.semaphore_signal(barrier, inc=1, device_id=device, device_id_type=MESH)

    def order(p):
        nearest = jnp.minimum(f, n_fs - 1 - f)
        step = (p + 1) // 2
        near = f + step if p % 2 else f - step
        far = f + (p - nearest) * jnp.where(2 * f < n_fs, 1, -1)
        return jnp.where(p <= 2 * nearest, near, far)

    def piece(g, j, q, c):
        buf = gathered[g][0]
        size = buf.shape[1] // n_rep // chunk_counts[g]
        start = pl.multiple_of((q * chunk_counts[g] + c) * size, size)
        return buf.at[j, pl.ds(start, size), :]

    def remote(g, j, q, c, send_slot, device):
        block = piece(g, j, q, c)
        sems = gathered[g][1]
        return pltpu.make_async_remote_copy(
            src_ref=block,
            dst_ref=block,
            send_sem=sems.at[j, send_slot, c],
            recv_sem=sems.at[j, q, c],
            device_id=device,
            device_id_type=MESH,
        )

    def along(g, j, c, way, act):
        if way == 0:

            @pl.when(f > 0)
            def _():
                act(remote(g, j, r, c, 2 * n_rep, {"fs": f - 1}))

        else:

            @pl.when(f < n_fs - 1)
            def _():
                act(remote(g, j, r, c, 2 * n_rep + 1, {"fs": f + 1}))

    def start(copy):
        copy.start()

    def drain(copy):
        copy.wait_send()

    def onward(g, p, c, act):
        j = order(p)

        @pl.when(j > f)
        def _():
            along(g, j, c, 0, act)

        @pl.when(j < f)
        def _():
            along(g, j, c, 1, act)

        for d in range(1, n_rep):
            other = lax.rem(r + d, n_rep)
            act(remote(g, j, r, c, n_rep + other, {"rep": other}))

    def send_own(g):
        for c in range(chunk_counts[g]):
            along(g, f, c, 0, start)
            along(g, f, c, 1, start)

    def relay(g, p):
        for c in range(chunk_counts[g]):
            j = order(p)
            remote(g, j, r, c, 2 * n_rep, {"fs": f}).wait_recv()
            onward(g, p, c, start)

    def arrived(g, p):
        j = order(p)
        for d in range(1, n_rep):
            other = lax.rem(r + d, n_rep)
            for c in range(chunk_counts[g]):
                remote(g, j, other, c, n_rep + other, {"rep": other}).wait_recv()

    def block_of(index):
        return pl.ds(pl.multiple_of(index * rows, rows), rows)

    def copy_to(source, target, send_sem, recv_sem, device):
        return pltpu.make_async_remote_copy(
            src_ref=source,
            dst_ref=target,
            send_sem=send_sem,
            recv_sem=recv_sem,
            device_id=device,
            device_id_type=MESH,
        )

    def tp_copies(kind, source, target):
        made = []
        for d in range(1, n_tp):
            other = lax.rem(t + d, n_tp)
            made.append(
                copy_to(
                    source(other),
                    target(t),
                    tp_send.at[kind, other],
                    tp_recv.at[kind, t],
                    {"tp": other},
                )
            )
        return made

    def tp_wait(kind, target):
        for d in range(1, n_tp):
            other = lax.rem(t + d, n_tp)
            copy_to(
                target(other),
                target(other),
                tp_send.at[kind, other],
                tp_recv.at[kind, other],
                {"tp": other},
            ).wait_recv()

    sends = []

    def send(copy):
        copy.start()
        sends.append(copy)

    def spread_rows(g, q, c):
        size = spread[g][0].shape[2] // n_rep // spread_counts[g]
        return pl.ds(pl.multiple_of((q * spread_counts[g] + c) * size, size), size)

    def source_of(d):
        return lax.rem(f - d + n_fs, n_fs)

    def spread_own(g, d):
        buf, stage, sems = spread[g]
        to = lax.rem(f + d, n_fs)
        for s in range(buf.shape[1]):
            for c in range(spread_counts[g]):
                piece = spread_rows(g, r, c)
                target = buf.at[f, s, piece, :]
                source = stage.at[s, piece, :] if d % 2 else target
                send(copy_to(source, target, sems.at[0, to, s, c], sems.at[1, f, s, c], {"fs": to}))

    def spread_relay(g, d, s):
        buf, _, sems = spread[g]
        j = source_of(d)
        for c in range(spread_counts[g]):
            block = buf.at[j, s, spread_rows(g, r, c), :]
            copy_to(block, block, sems.at[0, j, s, c], sems.at[1, j, s, c], {"fs": j}).wait_recv()
            for e in range(1, n_rep):
                other = lax.rem(r + e, n_rep)
                send(
                    copy_to(
                        block,
                        block,
                        sems.at[2 + other, j, s, c],
                        sems.at[2 + n_rep + r, j, s, c],
                        {"rep": other},
                    )
                )

    def spread_arrived(g, d, s):
        buf, _, sems = spread[g]
        j = source_of(d)
        for e in range(1, n_rep):
            other = lax.rem(r + e, n_rep)
            for c in range(spread_counts[g]):
                block = buf.at[j, s, spread_rows(g, other, c), :]
                copy_to(
                    block,
                    block,
                    sems.at[2 + other, j, s, c],
                    sems.at[2 + n_rep + other, j, s, c],
                    {"rep": other},
                ).wait_recv()

    stream = tokens[...].astype(jnp.float32)
    scale = lax.rsqrt(jnp.mean(stream * stream, axis=-1, keepdims=True) + epsilon)
    normed[block_of(t), :] = (stream * scale * gain1[...]).astype(jnp.bfloat16)

    pl.semaphore_wait(barrier, len(greeted))
    loads[0].wait()
    send_own(0)
    loads[1].wait()
    send_own(1)
    normed_at = lambda index: normed.at[block_of(index), :]
    for copy in tp_copies(0, lambda other: normed_at(t), normed_at):
        send(copy)
    for p in range(1, n_fs):
        relay(0, p)
        relay(1, p)
    loads[2].wait()
    loads[3].wait()
    for d in range(1, n_fs):
        spread_own(0, d)
    for copy in loads[4:]:
        copy.wait()
    spread_own(1, 1)

    tp_wait(0, normed_at)
    for p in range(1, n_fs):
        arrived(0, p)
    total = dot(normed[:, :part], in_buf[0])
    for index in range(1, n_fs):
        total += dot(normed[:, index * part : (index + 1) * part], in_buf[index])
    projected[...] = total.astype(jnp.bfloat16).astype(jnp.float32)
    groups, channels = group_weight.shape[0], group_weight.shape[1]
    position = lax.broadcasted_iota(jnp.int32, (length, channels), 0)
    for group in range(groups):
        lanes = slice(group * channels, (group + 1) * channels)
        values = projected[:, lanes]
        level_of = jnp.full((length, channels), lax.rem(t * groups + group, LEVELS), jnp.int32)
        running = values
        mean = jnp.zeros_like(values)
        for level in range(LEVELS):
            offset = 2**level
            running = running + jnp.where(position >= offset, pltpu.roll(running, offset, 0), 0.0)
            count = jnp.minimum(position + 1, 2 * offset).astype(jnp.float32)
            mean = jnp.where(level_of == level, running / count, mean)
        pooled = (mean - values).astype(jnp.bfloat16)
        mapped = dot(pooled, group_weight[group])
        pool_out[:, lanes] = (mapped * pool_scale[:, lanes]).astype(jnp.bfloat16)

    for p in range(1, n_fs):
        arrived(1, p)
    for index in range(n_fs):
        mix_send[index] = dot(pool_out[...], out_buf[index]).astype(jnp.bfloat16)
    for copy in tp_copies(
        1, lambda other: mix_send.at[:, block_of(other), :], lambda index: mix_recv.at[index]
    ):
        send(copy)
    for d in range(1, n_fs - 1):
        spread_relay(0, d, 0)

    tp_wait(1, lambda index: mix_recv.at[index])
    square = jnp.zeros((rows, 1), jnp.float32)
    for index in range(n_fs):
        mixed = tokens[:, index * part : (index + 1) * part].astype(jnp.float32)
        mixed += mix_send[index, block_of(t), :].astype(jnp.float32)
        for d in range(1, n_tp):
            mixed += mix_recv[lax.rem(t + d, n_tp), index].astype(jnp.float32)
        stream2[index] = mixed
        square += jnp.sum(mixed * mixed, axis=-1, keepdims=True)
    scale = lax.rsqrt(square / width + epsilon)

    def place_of(owner):
        return block_of(lax.rem(owner, 2) * n_y + owner // 2)

    for index in range(n_fs):
        columns = slice(index * part, (index + 1) * part)
        shared[half, place_of(t), columns] = (stream2[index] * scale * gain2[:, columns]).astype(
            jnp.bfloat16
        )

    def share(plane, owner, send_slot, device):
        block = shared.at[plane, place_of(owner), :]
        return copy_to(
            block, block, share_send.at[send_slot, plane, owner], share_recv.at[plane, owner], device
        )

    def share_core(plane, owner):
        send(share(plane, owner, n_y, {"tp": t_pair}))

    def on_line(e):
        return lax.rem(y + e, n_y)

    def share_line(plane):
        for e in range(1, n_y):
            to = on_line(e)
            send(share(plane, t, to, {"tp": 2 * to + core}))

    def shared_from(plane, owner):
        share(plane, owner, n_y, {"tp": t_pair}).wait_recv()

    def shared_by_core(plane):
        for e in range(n_y):
            shared_from(plane, 2 * on_line(e) + 1 - core)

    send(share(half, t, n_y + 1, {"fs": f_pair}))
    share_line(half)
    share_core(half, t)
    for d in range(2, n_fs):
        spread_own(1, d)
    spread_relay(0, n_fs - 1, 0)
    for e in range(1, n_y):
        owner = 2 * on_line(e) + core
        shared_from(half, owner)
        share_core(half, owner)
    shared_from(1 - half, t)
    share_line(1 - half)
    share_core(1 - half, t)
    shared_by_core(half)
    for d in range(1, n_fs):
        spread_arrived(0, d, 0)

    up_tile = tile_of(half_units, 256)

    def up_product(plane):
        @pl.loop(0, half_units // up_tile)
        def _(i):
            columns = pl.ds(pl.multiple_of(i * up_tile, up_tile), up_tile)
            total = dot(shared[plane, :, :part], up_buf[0, 0, :, columns])
            for index in range(1, n_fs):
                left = shared[plane, :, index * part : (index + 1) * part]
                total += dot(left, up_buf[index, 0, :, columns])
            value = jnp.maximum(total, 0.0)
            hidden[plane, :, columns] = (value * value).astype(jnp.bfloat16)

    up_product(half)
    for s in range(subs):
        spread_relay(1, 1, s)
    for e in range(1, n_y):
        owner = 2 * on_line(e) + core
        shared_from(1 - half, owner)
        share_core(1 - half, owner)
    shared_by_core(1 - half)
    up_product(1 - half)

    line_rows = n_y * rows

    def own_rows(which):
        return pl.ds(pl.multiple_of(which * line_rows, line_rows), line_rows)

    def down_product(k):
        d, s = k // subs, k % subs
        j = source_of(d)
        if d:
            spread_arrived(1, d, s)
        for plane in range(2):
            product = dot(hidden[plane], down_buf[j, s])
            core_send[k, plane] = product.astype(jnp.bfloat16)
        send(
            copy_to(
                core_send.at[k, :, own_rows(1 - core), :],
                core_recv.at[k],
                core_sems.at[0, k],
                core_sems.at[1, k],
                {"tp": t_pair},
            )
        )

    def to_line(k):
        copy_to(
            core_recv.at[k], core_recv.at[k], core_sems.at[0, k], core_sems.at[1, k], {"tp": t_pair}
        ).wait_recv()
        for plane in range(2):
            own = core_send[k, plane, own_rows(core), :].astype(jnp.float32)
            both = own + core_recv[k, plane].astype(jnp.float32)
            line_send[k, plane] = both.astype(jnp.bfloat16)
        for e in range(1, n_y):
            to = on_line(e)
            send(
                copy_to(
                    line_send.at[k, :, block_of(to), :],
                    line_recv.at[k, y],
                    line_sems.at[0, k, to],
                    line_sems.at[1, k, y],
                    {"tp": 2 * to + core},
                )
            )

    def to_pair(k):
        d, s = k // subs, k % subs
        j = source_of(d)
        for e in range(1, n_y):
            block = line_recv.at[k, on_line(e)]
            copy_to(
                block,
                block,
                line_sems.at[0, k, on_line(e)],
                line_sems.at[1, k, on_line(e)],
                {"tp": t_pair},
            ).wait_recv()

        def total_of(plane):
            total = core_send[k, plane, block_of(core * n_y + y), :].astype(jnp.float32)
            total += core_recv[k, plane, block_of(y), :].astype(jnp.float32)
            for e in range(1, n_y):
                total += line_recv[k, on_line(e), plane].astype(jnp.float32)
            return total

        pair_send[j * subs + s] = total_of(1 - half).astype(jnp.bfloat16)
        send(
            copy_to(
                pair_send.at[j * subs + s],
                pair_recv.at[j * subs + s],
                pair_sems.at[0, j * subs + s],
                pair_sems.at[1, j * subs + s],
                {"fs": f_pair},
            )
        )
        columns = slice(s * sub_columns, (s + 1) * sub_columns)
        stream2[j, :, columns] += total_of(half)

    def finish(k):
        d, s = k // subs, k % subs
        j = lax.rem(f - half - d + n_fs, n_fs)
        slot = j * subs + s
        copy_to(
            pair_recv.at[slot],
            pair_recv.at[slot],
            pair_sems.at[0, slot],
            pair_sems.at[1, slot],
            {"fs": f_pair},
        ).wait_recv()
        columns = slice(s * sub_columns, (s + 1) * sub_columns)
        value = stream2[j, :, columns] + pair_recv[slot].astype(jnp.float32)
        target = pl.ds(pl.multiple_of(j * part + s * sub_columns, sub_columns), sub_columns)
        result[:, target] = value.astype(jnp.bfloat16)

    for k in range(steps + 3 + subs):
        if 2 * subs <= k + 1 < steps:
            spread_relay(1, (k + 1) // subs, (k + 1) % subs)
        if k < steps:
            down_product(k)
        if 0 <= k - 1 < steps:
            to_line(k - 1)
        if 0 <= k - 2 < steps:
            to_pair(k - 2)
        if 0 <= k - 3 - subs < steps:
            finish(k - 3 - subs)

    for g in range(2):
        for c in range(chunk_counts[g]):
            along(g, f, c, 0, drain)
            along(g, f, c, 1, drain)
            for p in range(1, n_fs):
                onward(g, p, c, drain)
    for copy in sends:
        copy.wait_send()


def local(sizes, tokens, gain1, in_w, group_w, pool_scale, out_w, gain2, up_w, down_w):
    n_rep, n_fs, n_tp = sizes
    n_y = n_tp // 2
    rows, width = tokens.shape
    length, part = rows * n_tp, width // n_fs
    channels, half_units = in_w.shape[1], up_w.shape[1] // 2
    sub_columns = tile_of(part, SUB_COLUMNS)
    subs = part // sub_columns
    steps = n_fs * subs
    bf16, f32 = jnp.bfloat16, jnp.float32
    vmem = pl.BlockSpec(memory_space=pltpu.VMEM)
    hbm = pl.BlockSpec(memory_space=pl.ANY)
    dma = pltpu.SemaphoreType.DMA
    kinds = 2 + 2 * n_rep
    return pl.pallas_call(
        functools.partial(kernel, sizes),
        name="layer",
        out_shape=jax.ShapeDtypeStruct((rows, width), bf16),
        in_specs=[vmem, vmem, hbm, vmem, vmem, hbm, vmem, hbm, hbm],
        out_specs=vmem,
        scratch_shapes=[
            pltpu.VMEM((n_fs,) + in_w.shape, bf16),
            pltpu.VMEM((n_fs,) + out_w.shape, bf16),
            pltpu.VMEM((n_fs, 1, part, half_units), bf16),
            pltpu.VMEM((n_fs, subs, half_units, sub_columns), bf16),
            pltpu.VMEM((1, part, half_units), bf16),
            pltpu.VMEM((subs, half_units, sub_columns), bf16),
            pltpu.VMEM((length, width), bf16),
            pltpu.VMEM((length, channels), f32),
            pltpu.VMEM((length, channels), bf16),
            pltpu.VMEM((n_fs, length, part), bf16),
            pltpu.VMEM((n_tp, n_fs, rows, part), bf16),
            pltpu.VMEM((n_fs, rows, part), f32),
            pltpu.VMEM((2, length, width), bf16),
            pltpu.VMEM((2, length, half_units), bf16),
            pltpu.VMEM((steps, 2, length, sub_columns), bf16),
            pltpu.VMEM((steps, 2, n_y * rows, sub_columns), bf16),
            pltpu.VMEM((steps, 2, n_y * rows, sub_columns), bf16),
            pltpu.VMEM((steps, n_y, 2, rows, sub_columns), bf16),
            pltpu.VMEM((steps, rows, sub_columns), bf16),
            pltpu.VMEM((steps, rows, sub_columns), bf16),
            dma((4 + 2 * subs,)),
            dma((n_fs, 2 * n_rep + 2, chunks_of(*in_w.shape, n_rep))),
            dma((n_fs, 2 * n_rep + 2, chunks_of(*out_w.shape, n_rep))),
            dma((kinds, n_fs, 1, chunks_of(part, half_units, n_rep))),
            dma((kinds, n_fs, subs, chunks_of(half_units, sub_columns, n_rep))),
            dma((2, n_tp)),
            dma((2, n_tp)),
            dma((n_y + 2, 2, n_tp)),
            dma((2, n_tp)),
            dma((2, steps)),
            dma((2, steps, n_y)),
            dma((2, steps)),
        ],
        compiler_params=pltpu.CompilerParams(
            collective_id=0, has_side_effects=True, vmem_limit_bytes=60 * 1024 * 1024
        ),
    )(
        tokens,
        gain1.reshape(1, -1),
        in_w,
        group_w,
        pool_scale.reshape(1, -1),
        out_w,
        gain2.reshape(1, -1),
        up_w,
        down_w,
    )


def solution(mesh):
    sizes = tuple(mesh.shape[axis] for axis in ("rep", "fs", "tp"))
    in_specs = (
        P(("rep", "fs", "tp"), None),
        P(),
        P("fs", "tp"),
        P("tp", None, None),
        P("tp"),
        P("tp", "fs"),
        P(),
        P("fs", "tp"),
        P("tp", "fs"),
    )
    return jax.shard_map(
        functools.partial(local, sizes),
        mesh=mesh,
        in_specs=in_specs,
        out_specs=P(("rep", "fs", "tp"), None),
        check_vma=False,
    )
```

```python
import functools

import jax
import jax.numpy as jnp
from jax import lax
from jax.experimental import pallas as pl
from jax.experimental.pallas import tpu as pltpu
from jax.sharding import PartitionSpec as P

MESH = pl.DeviceIdType.MESH
CHUNK_BYTES = 128 * 1024
SUB_COLUMNS = 256
SHARE_CHUNKS = 4
LEVELS = 4

epsilon = 1e-06


def chunks_of(rows, columns, parts):
    count = max(1, rows * columns * 2 // parts // CHUNK_BYTES)
    while (rows // parts) % (count * 16):
        count -= 1
    return count


def dot(a, b):
    return jnp.dot(a, b, preferred_element_type=jnp.float32)


def tile_of(columns, most):
    tile = min(columns, most)
    while columns % tile:
        tile //= 2
    return tile


def kernel(
    sizes,
    tokens,
    gain1,
    in_hbm,
    group_weight,
    pool_scale,
    out_hbm,
    gain2,
    up_hbm,
    down_hbm,
    result,
    in_buf,
    out_buf,
    up_buf,
    down_buf,
    normed,
    projected,
    pool_out,
    mix_send,
    mix_core,
    mix_line_send,
    mix_line,
    stream2,
    shared,
    hidden,
    core_send,
    core_recv,
    line_send,
    line_recv,
    pair_send,
    pair_recv,
    local_sem,
    in_sems,
    out_sems,
    up_sems,
    down_sems,
    normed_send,
    normed_recv,
    mix_core_sems,
    mix_line_sems,
    share_send,
    share_recv,
    core_sems,
    line_sems,
    pair_sems,
):
    n_rep, n_fs, n_tp = sizes
    n_y = n_tp // 2
    r, f, t = lax.axis_index("rep"), lax.axis_index("fs"), lax.axis_index("tp")
    core, y = lax.rem(t, 2), t // 2
    half = lax.rem(f, 2)
    f_pair, t_pair = f + 1 - 2 * half, t + 1 - 2 * core
    rows = tokens.shape[0]
    length = rows * n_tp
    width = tokens.shape[1]
    part = width // n_fs
    subs = down_buf.shape[1]
    sub_columns = down_buf.shape[3]
    steps = n_fs * subs
    half_units = up_buf.shape[3]
    gathered = ((in_buf, in_sems), (out_buf, out_sems))
    chunk_counts = [chunks_of(b.shape[1], b.shape[2], n_rep) for b, _ in gathered]
    spread = ((up_buf, up_sems), (down_buf, down_sems))
    spread_counts = [chunks_of(b.shape[2], b.shape[3], n_rep) for b, _ in spread]

    loads = []

    def load(source, target):
        copy = pltpu.make_async_copy(source, target, local_sem.at[len(loads)])
        copy.start()
        loads.append(copy)

    def units_of(which):
        return pl.ds(pl.multiple_of(which * half_units, half_units), half_units)

    load(in_hbm, in_buf.at[f])
    load(out_hbm, out_buf.at[f])
    load(up_hbm.at[:, units_of(1 - half)], up_buf.at[n_fs, 0])
    load(up_hbm.at[:, units_of(half)], up_buf.at[f, 0])
    for s in range(subs):
        columns = pl.ds(s * sub_columns, sub_columns)
        load(down_hbm.at[units_of(1 - half), columns], down_buf.at[n_fs, s])
        load(down_hbm.at[units_of(half), columns], down_buf.at[f, s])

    barrier = pltpu.get_barrier_semaphore()
    greeted = [{"fs": lax.rem(f + d, n_fs)} for d in range(1, n_fs)]
    greeted += [{"rep": lax.rem(r + d, n_rep)} for d in range(1, n_rep)]
    greeted += [{"tp": lax.rem(t + d, n_tp)} for d in range(1, n_tp)]
    for device in greeted:
        pl.semaphore_signal(barrier, inc=1, device_id=device, device_id_type=MESH)

    inward = jnp.where(2 * f < n_fs, 1, -1)

    def order(p):
        nearest = jnp.minimum(f, n_fs - 1 - f)
        step = (p + 1) // 2
        near = f + step * inward if p % 2 else f - step * inward
        far = f + (p - nearest) * inward
        return jnp.where(p <= 2 * nearest, near, far)

    def piece(g, j, q, c):
        buf = gathered[g][0]
        size = buf.shape[1] // n_rep // chunk_counts[g]
        start = pl.multiple_of((q * chunk_counts[g] + c) * size, size)
        return buf.at[j, pl.ds(start, size), :]

    def remote(g, j, q, c, send_slot, device):
        block = piece(g, j, q, c)
        sems = gathered[g][1]
        return pltpu.make_async_remote_copy(
            src_ref=block,
            dst_ref=block,
            send_sem=sems.at[j, send_slot, c],
            recv_sem=sems.at[j, q, c],
            device_id=device,
            device_id_type=MESH,
        )

    def along(g, j, c, way, act):
        if way == 0:

            @pl.when(f > 0)
            def _():
                act(remote(g, j, r, c, 2 * n_rep, {"fs": f - 1}))

        else:

            @pl.when(f < n_fs - 1)
            def _():
                act(remote(g, j, r, c, 2 * n_rep + 1, {"fs": f + 1}))

    def start(copy):
        copy.start()

    def drain(copy):
        copy.wait_send()

    def onward(g, p, c, act):
        j = order(p)

        @pl.when(j > f)
        def _():
            along(g, j, c, 0, act)

        @pl.when(j < f)
        def _():
            along(g, j, c, 1, act)

        for d in range(1, n_rep):
            other = lax.rem(r + d, n_rep)
            act(remote(g, j, r, c, n_rep + other, {"rep": other}))

    def send_own(g):
        for c in range(chunk_counts[g]):
            along(g, f, c, 0, start)
            along(g, f, c, 1, start)

    def relay(g, p):
        for c in range(chunk_counts[g]):
            j = order(p)
            remote(g, j, r, c, 2 * n_rep, {"fs": f}).wait_recv()
            onward(g, p, c, start)

    def arrived(g, p):
        j = order(p)
        for d in range(1, n_rep):
            other = lax.rem(r + d, n_rep)
            for c in range(chunk_counts[g]):
                remote(g, j, other, c, n_rep + other, {"rep": other}).wait_recv()

    def block_of(index):
        return pl.ds(pl.multiple_of(index * rows, rows), rows)

    def copy_to(source, target, send_sem, recv_sem, device):
        return pltpu.make_async_remote_copy(
            src_ref=source,
            dst_ref=target,
            send_sem=send_sem,
            recv_sem=recv_sem,
            device_id=device,
            device_id_type=MESH,
        )

    sends = []

    def send(copy):
        copy.start()
        sends.append(copy)

    def spread_rows(g, q, c):
        size = spread[g][0].shape[2] // n_rep // spread_counts[g]
        return pl.ds(pl.multiple_of((q * spread_counts[g] + c) * size, size), size)

    farthest = list(range(n_fs - 1, 0, -1))
    at_end = jnp.logical_or(f == 0, f == n_fs - 1)

    def by_place(ends, k):
        return jnp.where(at_end, order(ends[k - 1]), order(farthest[k - 1]))

    def ranked(k):
        return by_place([1] + farthest[:-1], k) if k else f

    def sent(k):
        return by_place(farthest[1:2] + farthest[:1] + farthest[2:], k)

    def spread_own(g, act):
        buf, sems = spread[g]
        for k in range(1, n_fs):
            to = sent(k)
            slot = jnp.where(lax.rem(to, 2) == half, f, n_fs)
            for s in range(buf.shape[1]):
                for c in range(spread_counts[g]):
                    piece = spread_rows(g, r, c)
                    act(
                        copy_to(
                            buf.at[slot, s, piece, :],
                            buf.at[f, s, piece, :],
                            sems.at[0, to, s, c],
                            sems.at[1, f, s, c],
                            {"fs": to},
                        )
                    )

    def spread_relay(g, k, s):
        buf, sems = spread[g]
        j = ranked(k)
        for c in range(spread_counts[g]):
            block = buf.at[j, s, spread_rows(g, r, c), :]
            copy_to(block, block, sems.at[0, j, s, c], sems.at[1, j, s, c], {"fs": j}).wait_recv()
            for e in range(1, n_rep):
                other = lax.rem(r + e, n_rep)
                send(
                    copy_to(
                        block,
                        block,
                        sems.at[2 + other, j, s, c],
                        sems.at[2 + n_rep + r, j, s, c],
                        {"rep": other},
                    )
                )

    def spread_arrived(g, k, s):
        buf, sems = spread[g]
        j = ranked(k)
        for e in range(1, n_rep):
            other = lax.rem(r + e, n_rep)
            for c in range(spread_counts[g]):
                block = buf.at[j, s, spread_rows(g, other, c), :]
                copy_to(
                    block,
                    block,
                    sems.at[2 + other, j, s, c],
                    sems.at[2 + n_rep + other, j, s, c],
                    {"rep": other},
                ).wait_recv()

    stream = tokens[...].astype(jnp.float32)
    scale = lax.rsqrt(jnp.mean(stream * stream, axis=-1, keepdims=True) + epsilon)
    normed[block_of(t), :] = (stream * scale * gain1[...]).astype(jnp.bfloat16)

    def on_line(e):
        return lax.rem(y + e, n_y)

    def give_normed(owner, slot, device):
        block = normed.at[block_of(owner), :]
        return copy_to(block, block, normed_send.at[slot, owner], normed_recv.at[owner], device)

    def normed_from(owner):
        give_normed(owner, n_y, {"tp": t_pair}).wait_recv()

    pl.semaphore_wait(barrier, len(greeted))
    for e in range(1, n_y):
        to = on_line(e)
        send(give_normed(t, to, {"tp": 2 * to + core}))
    send(give_normed(t, n_y, {"tp": t_pair}))
    loads[0].wait()
    send_own(0)
    loads[1].wait()
    send_own(1)
    for p in range(1, n_fs):
        relay(0, p)
    for p in range(1, n_fs):
        relay(1, p)
    for e in range(1, n_y):
        owner = 2 * on_line(e) + core
        normed_from(owner)
        send(give_normed(owner, n_y, {"tp": t_pair}))
    for copy in loads[2:]:
        copy.wait()

    @pl.when(at_end)
    def _():
        spread_own(0, start)

    for p in range(1, n_fs):
        arrived(0, p)
    for e in range(n_y):
        normed_from(2 * on_line(e) + 1 - core)
    total = dot(normed[:, :part], in_buf[0])
    for index in range(1, n_fs):
        total += dot(normed[:, index * part : (index + 1) * part], in_buf[index])
    projected[...] = total.astype(jnp.bfloat16).astype(jnp.float32)
    groups, channels = group_weight.shape[0], group_weight.shape[1]
    position = lax.broadcasted_iota(jnp.int32, (length, channels), 0)
    for group in range(groups):
        lanes = slice(group * channels, (group + 1) * channels)
        values = projected[:, lanes]
        level_of = jnp.full((length, channels), lax.rem(t * groups + group, LEVELS), jnp.int32)
        running = values
        mean = jnp.zeros_like(values)
        for level in range(LEVELS):
            offset = 2**level
            running = running + jnp.where(position >= offset, pltpu.roll(running, offset, 0), 0.0)
            count = jnp.minimum(position + 1, 2 * offset).astype(jnp.float32)
            mean = jnp.where(level_of == level, running / count, mean)
        pooled = (mean - values).astype(jnp.bfloat16)
        mapped = dot(pooled, group_weight[group])
        pool_out[:, lanes] = (mapped * pool_scale[:, lanes]).astype(jnp.bfloat16)


    @pl.when(jnp.logical_not(at_end))
    def _():
        spread_own(0, start)

    for p in range(1, n_fs):
        arrived(1, p)
    def mix_by_core(index, e):
        block = mix_send.at[index, block_of(2 * e + 1 - core), :]
        sems = mix_core_sems
        return copy_to(
            block, mix_core.at[index, e], sems.at[0, index, e], sems.at[1, index, e], {"tp": t_pair}
        )

    def mix_by_line(index, source, target, to):
        sems = mix_line_sems
        return copy_to(
            source, target, sems.at[0, index, to], sems.at[1, index, y], {"tp": 2 * to + core}
        )

    def mix_pair(index, which):
        own = mix_send[index, block_of(2 * which + core), :].astype(jnp.float32)
        return own + mix_core[index, which].astype(jnp.float32)

    for index in range(n_fs):
        mix_send[index] = dot(pool_out[...], out_buf[index]).astype(jnp.bfloat16)
        for e in range(n_y):
            send(mix_by_core(index, e))
    for index in range(n_fs):
        for e in range(n_y):
            mix_by_core(index, e).wait_recv()
        for e in range(1, n_y):
            to = on_line(e)
            mix_line_send[index, to] = mix_pair(index, to).astype(jnp.bfloat16)
            send(mix_by_line(index, mix_line_send.at[index, to], mix_line.at[index, y], to))

    spread_relay(0, 1, 0)
    square = jnp.zeros((rows, 1), jnp.float32)
    for index in range(n_fs):
        mixed = tokens[:, index * part : (index + 1) * part].astype(jnp.float32)
        mixed += mix_pair(index, y)
        for e in range(1, n_y):
            block = mix_line.at[index, on_line(e)]
            copy_to(
                block,
                block,
                mix_line_sems.at[0, index, on_line(e)],
                mix_line_sems.at[1, index, on_line(e)],
                {"tp": t_pair},
            ).wait_recv()
            mixed += block[...].astype(jnp.float32)
        stream2[index] = mixed
        square += jnp.sum(mixed * mixed, axis=-1, keepdims=True)
    scale = lax.rsqrt(square / width + epsilon)

    def place_of(owner):
        return block_of(lax.rem(owner, 2) * n_y + owner // 2)

    for index in range(n_fs):
        columns = slice(index * part, (index + 1) * part)
        shared[half, place_of(t), columns] = (stream2[index] * scale * gain2[:, columns]).astype(
            jnp.bfloat16
        )

    def share(plane, owner, c, send_slot, device):
        size = rows // SHARE_CHUNKS
        place = lax.rem(owner, 2) * n_y + owner // 2
        start = pl.multiple_of(place * rows + c * size, size)
        block = shared.at[plane, pl.ds(start, size), :]
        return copy_to(
            block,
            block,
            share_send.at[send_slot, plane, owner, c],
            share_recv.at[plane, owner, c],
            device,
        )

    def share_core(plane, owner, c):
        send(share(plane, owner, c, n_y, {"tp": t_pair}))

    def share_line(plane, c):
        for e in range(1, n_y):
            to = on_line(e)
            send(share(plane, t, c, to, {"tp": 2 * to + core}))

    def shared_from(plane, owner, c):
        share(plane, owner, c, n_y, {"tp": t_pair}).wait_recv()

    def shared_by_core(plane):
        for e in range(n_y):
            for c in range(SHARE_CHUNKS):
                shared_from(plane, 2 * on_line(e) + 1 - core, c)

    for c in range(SHARE_CHUNKS):
        send(share(half, t, c, n_y + 1, {"fs": f_pair}))
        share_line(half, c)
        share_core(half, t, c)
    spread_own(1, start)
    for c in range(SHARE_CHUNKS):
        for e in range(1, n_y):
            owner = 2 * on_line(e) + core
            shared_from(half, owner, c)
            share_core(half, owner, c)
    for k in range(2, n_fs - 1):
        spread_relay(0, k, 0)
    for c in range(SHARE_CHUNKS):
        shared_from(1 - half, t, c)
        share_line(1 - half, c)
        share_core(1 - half, t, c)
    spread_relay(0, n_fs - 1, 0)
    for c in range(SHARE_CHUNKS):
        for e in range(1, n_y):
            owner = 2 * on_line(e) + core
            shared_from(1 - half, owner, c)
            share_core(1 - half, owner, c)
    shared_by_core(half)
    spread_relay(1, 1, 0)
    for d in range(1, n_fs):
        spread_arrived(0, d, 0)

    up_tile = tile_of(half_units, 256)

    def up_product(plane):
        @pl.loop(0, half_units // up_tile)
        def _(i):
            columns = pl.ds(pl.multiple_of(i * up_tile, up_tile), up_tile)
            total = dot(shared[plane, :, :part], up_buf[0, 0, :, columns])
            for index in range(1, n_fs):
                left = shared[plane, :, index * part : (index + 1) * part]
                total += dot(left, up_buf[index, 0, :, columns])
            value = jnp.maximum(total, 0.0)
            hidden[plane, :, columns] = (value * value).astype(jnp.bfloat16)

    up_product(half)
    for s in range(1, subs):
        spread_relay(1, 1, s)
    shared_by_core(1 - half)
    up_product(1 - half)

    line_rows = n_y * rows

    def own_rows(which):
        return pl.ds(pl.multiple_of(which * line_rows, line_rows), line_rows)

    def down_product(k):
        d, s = k // subs, k % subs
        j = ranked(d)
        if d:
            spread_arrived(1, d, s)
        for plane in range(2):
            product = dot(hidden[plane], down_buf[j, s])
            core_send[k, plane] = product.astype(jnp.bfloat16)
        send(
            copy_to(
                core_send.at[k, :, own_rows(1 - core), :],
                core_recv.at[k],
                core_sems.at[0, k],
                core_sems.at[1, k],
                {"tp": t_pair},
            )
        )

    def to_line(k):
        copy_to(
            core_recv.at[k], core_recv.at[k], core_sems.at[0, k], core_sems.at[1, k], {"tp": t_pair}
        ).wait_recv()
        for plane in range(2):
            own = core_send[k, plane, own_rows(core), :].astype(jnp.float32)
            both = own + core_recv[k, plane].astype(jnp.float32)
            line_send[k, plane] = both.astype(jnp.bfloat16)
        for e in range(1, n_y):
            to = on_line(e)
            send(
                copy_to(
                    line_send.at[k, :, block_of(to), :],
                    line_recv.at[k, y],
                    line_sems.at[0, k, to],
                    line_sems.at[1, k, y],
                    {"tp": 2 * to + core},
                )
            )

    def to_pair(k):
        d, s = k // subs, k % subs
        j = ranked(d)
        for e in range(1, n_y):
            block = line_recv.at[k, on_line(e)]
            copy_to(
                block,
                block,
                line_sems.at[0, k, on_line(e)],
                line_sems.at[1, k, on_line(e)],
                {"tp": t_pair},
            ).wait_recv()

        def total_of(plane):
            total = core_send[k, plane, block_of(core * n_y + y), :].astype(jnp.float32)
            total += core_recv[k, plane, block_of(y), :].astype(jnp.float32)
            for e in range(1, n_y):
                total += line_recv[k, on_line(e), plane].astype(jnp.float32)
            return total

        pair_send[j * subs + s] = total_of(1 - half).astype(jnp.bfloat16)
        send(
            copy_to(
                pair_send.at[j * subs + s],
                pair_recv.at[j * subs + s],
                pair_sems.at[0, j * subs + s],
                pair_sems.at[1, j * subs + s],
                {"fs": f_pair},
            )
        )
        columns = slice(s * sub_columns, (s + 1) * sub_columns)
        stream2[j, :, columns] += total_of(half)

    def finish(k):
        d, s = k // subs, k % subs
        j = ranked(d)
        slot = j * subs + s
        copy_to(
            pair_recv.at[slot],
            pair_recv.at[slot],
            pair_sems.at[0, slot],
            pair_sems.at[1, slot],
            {"fs": f_pair},
        ).wait_recv()
        columns = slice(s * sub_columns, (s + 1) * sub_columns)
        value = stream2[j, :, columns] + pair_recv[slot].astype(jnp.float32)
        target = pl.ds(pl.multiple_of(j * part + s * sub_columns, sub_columns), sub_columns)
        result[:, target] = value.astype(jnp.bfloat16)

    for k in range(steps + 4):
        if 2 * subs <= k + 1 < steps:
            spread_relay(1, (k + 1) // subs, (k + 1) % subs)
        if k < steps:
            down_product(k)
        if 0 <= k - 1 < steps:
            to_line(k - 1)
        if 0 <= k - 4 < steps:
            to_pair(k - 4)
    for k in range(steps):
        finish(k)

    for g in range(2):
        for c in range(chunk_counts[g]):
            along(g, f, c, 0, drain)
            along(g, f, c, 1, drain)
            for p in range(1, n_fs):
                onward(g, p, c, drain)
    for g in range(2):
        spread_own(g, drain)
    for copy in sends:
        copy.wait_send()


def local(sizes, tokens, gain1, in_w, group_w, pool_scale, out_w, gain2, up_w, down_w):
    n_rep, n_fs, n_tp = sizes
    n_y = n_tp // 2
    rows, width = tokens.shape
    length, part = rows * n_tp, width // n_fs
    channels, half_units = in_w.shape[1], up_w.shape[1] // 2
    sub_columns = tile_of(part, SUB_COLUMNS)
    subs = part // sub_columns
    steps = n_fs * subs
    bf16, f32 = jnp.bfloat16, jnp.float32
    vmem = pl.BlockSpec(memory_space=pltpu.VMEM)
    hbm = pl.BlockSpec(memory_space=pl.ANY)
    dma = pltpu.SemaphoreType.DMA
    kinds = 2 + 2 * n_rep
    return pl.pallas_call(
        functools.partial(kernel, sizes),
        name="layer",
        out_shape=jax.ShapeDtypeStruct((rows, width), bf16),
        in_specs=[vmem, vmem, hbm, vmem, vmem, hbm, vmem, hbm, hbm],
        out_specs=vmem,
        scratch_shapes=[
            pltpu.VMEM((n_fs,) + in_w.shape, bf16),
            pltpu.VMEM((n_fs,) + out_w.shape, bf16),
            pltpu.VMEM((n_fs + 1, 1, part, half_units), bf16),
            pltpu.VMEM((n_fs + 1, subs, half_units, sub_columns), bf16),
            pltpu.VMEM((length, width), bf16),
            pltpu.VMEM((length, channels), f32),
            pltpu.VMEM((length, channels), bf16),
            pltpu.VMEM((n_fs, length, part), bf16),
            pltpu.VMEM((n_fs, n_y, rows, part), bf16),
            pltpu.VMEM((n_fs, n_y, rows, part), bf16),
            pltpu.VMEM((n_fs, n_y, rows, part), bf16),
            pltpu.VMEM((n_fs, rows, part), f32),
            pltpu.VMEM((2, length, width), bf16),
            pltpu.VMEM((2, length, half_units), bf16),
            pltpu.VMEM((steps, 2, length, sub_columns), bf16),
            pltpu.VMEM((steps, 2, n_y * rows, sub_columns), bf16),
            pltpu.VMEM((steps, 2, n_y * rows, sub_columns), bf16),
            pltpu.VMEM((steps, n_y, 2, rows, sub_columns), bf16),
            pltpu.VMEM((steps, rows, sub_columns), bf16),
            pltpu.VMEM((steps, rows, sub_columns), bf16),
            dma((4 + 2 * subs,)),
            dma((n_fs, 2 * n_rep + 2, chunks_of(*in_w.shape, n_rep))),
            dma((n_fs, 2 * n_rep + 2, chunks_of(*out_w.shape, n_rep))),
            dma((kinds, n_fs, 1, chunks_of(part, half_units, n_rep))),
            dma((kinds, n_fs, subs, chunks_of(half_units, sub_columns, n_rep))),
            dma((n_y + 1, n_tp)),
            dma((n_tp,)),
            dma((2, n_fs, n_y)),
            dma((2, n_fs, n_y)),
            dma((n_y + 2, 2, n_tp, SHARE_CHUNKS)),
            dma((2, n_tp, SHARE_CHUNKS)),
            dma((2, steps)),
            dma((2, steps, n_y)),
            dma((2, steps)),
        ],
        compiler_params=pltpu.CompilerParams(
            collective_id=0, has_side_effects=True, vmem_limit_bytes=60 * 1024 * 1024
        ),
    )(
        tokens,
        gain1.reshape(1, -1),
        in_w,
        group_w,
        pool_scale.reshape(1, -1),
        out_w,
        gain2.reshape(1, -1),
        up_w,
        down_w,
    )


def solution(mesh):
    sizes = tuple(mesh.shape[axis] for axis in ("rep", "fs", "tp"))
    in_specs = (
        P(("rep", "fs", "tp"), None),
        P(),
        P("fs", "tp"),
        P("tp", None, None),
        P("tp"),
        P("tp", "fs"),
        P(),
        P("fs", "tp"),
        P("tp", "fs"),
    )
    return jax.shard_map(
        functools.partial(local, sizes),
        mesh=mesh,
        in_specs=in_specs,
        out_specs=P(("rep", "fs", "tp"), None),
        check_vma=False,
    )
```

```python
import functools

import jax
import jax.numpy as jnp
from jax import lax
from jax.experimental import pallas as pl
from jax.experimental.pallas import tpu as pltpu
from jax.sharding import PartitionSpec as P

MESH = pl.DeviceIdType.MESH
CHUNK_BYTES = 128 * 1024
SUB_COLUMNS = 128
AHEAD = 4
SHARE_CHUNKS = 4
LEVELS = 4

epsilon = 1e-06


def chunks_of(rows, columns, parts):
    count = max(1, rows * columns * 2 // parts // CHUNK_BYTES)
    while (rows // parts) % (count * 16):
        count -= 1
    return count


def dot(a, b):
    return jnp.dot(a, b, preferred_element_type=jnp.float32)


def tile_of(columns, most):
    tile = min(columns, most)
    while columns % tile:
        tile //= 2
    return tile


def kernel(
    sizes,
    tokens,
    gain1,
    in_hbm,
    group_weight,
    pool_scale,
    out_hbm,
    gain2,
    up_hbm,
    down_hbm,
    result,
    in_buf,
    out_buf,
    up_buf,
    down_buf,
    normed,
    projected,
    pool_out,
    mix_send,
    mix_core,
    mix_line_send,
    mix_line,
    stream2,
    shared,
    hidden,
    core_send,
    core_recv,
    line_send,
    line_recv,
    pair_send,
    pair_recv,
    local_sem,
    in_sems,
    out_sems,
    up_arrivals,
    up_swaps,
    up_sent,
    down_arrivals,
    down_swaps,
    down_sent,
    normed_send,
    normed_recv,
    mix_sent,
    mix_core_sems,
    mix_line_sems,
    share_sent,
    share_core_sems,
    share_line_sems,
    share_pair_sems,
    sums_sent,
    core_sems,
    line_sems,
    pair_sems,
):
    n_rep, n_fs, n_tp = sizes
    n_y = n_tp // 2
    r, f, t = lax.axis_index("rep"), lax.axis_index("fs"), lax.axis_index("tp")
    core, y = lax.rem(t, 2), t // 2
    half = lax.rem(f, 2)
    f_pair, t_pair = f + 1 - 2 * half, t + 1 - 2 * core
    rows = tokens.shape[0]
    length = rows * n_tp
    width = tokens.shape[1]
    part = width // n_fs
    subs = down_buf.shape[1]
    sub_columns = down_buf.shape[3]
    steps = n_fs * subs
    half_units = up_buf.shape[3]
    gathered = ((in_buf, in_sems), (out_buf, out_sems))
    chunk_counts = [chunks_of(b.shape[1], b.shape[2], n_rep) for b, _ in gathered]
    spread = (
        (up_buf, up_arrivals, up_swaps, up_sent),
        (down_buf, down_arrivals, down_swaps, down_sent),
    )
    spread_counts = [chunks_of(item[0].shape[2], item[0].shape[3], n_rep) for item in spread]

    loads = []

    def load(source, target):
        copy = pltpu.make_async_copy(source, target, local_sem.at[len(loads)])
        copy.start()
        loads.append(copy)

    def units_of(which):
        return pl.ds(pl.multiple_of(which * half_units, half_units), half_units)

    load(in_hbm, in_buf.at[f])
    load(out_hbm, out_buf.at[f])
    load(up_hbm.at[:, units_of(1 - half)], up_buf.at[n_fs, 0])
    load(up_hbm.at[:, units_of(half)], up_buf.at[f, 0])
    for s in range(subs):
        columns = pl.ds(s * sub_columns, sub_columns)
        load(down_hbm.at[units_of(1 - half), columns], down_buf.at[n_fs, s])
        load(down_hbm.at[units_of(half), columns], down_buf.at[f, s])

    barrier = pltpu.get_barrier_semaphore()
    greeted = [{"fs": lax.rem(f + d, n_fs)} for d in range(1, n_fs)]
    greeted += [{"rep": lax.rem(r + d, n_rep)} for d in range(1, n_rep)]
    greeted += [{"tp": lax.rem(t + d, n_tp)} for d in range(1, n_tp)]
    for device in greeted:
        pl.semaphore_signal(barrier, inc=1, device_id=device, device_id_type=MESH)

    inward = jnp.where(2 * f < n_fs, 1, -1)

    def order(p):
        nearest = jnp.minimum(f, n_fs - 1 - f)
        step = (p + 1) // 2
        near = f + step * inward if p % 2 else f - step * inward
        far = f + (p - nearest) * inward
        return jnp.where(p <= 2 * nearest, near, far)

    def piece(g, j, q, c):
        buf = gathered[g][0]
        size = buf.shape[1] // n_rep // chunk_counts[g]
        start = pl.multiple_of((q * chunk_counts[g] + c) * size, size)
        return buf.at[j, pl.ds(start, size), :]

    def remote(g, j, q, c, send_slot, device):
        block = piece(g, j, q, c)
        sems = gathered[g][1]
        return pltpu.make_async_remote_copy(
            src_ref=block,
            dst_ref=block,
            send_sem=sems.at[j, send_slot, c],
            recv_sem=sems.at[j, q, c],
            device_id=device,
            device_id_type=MESH,
        )

    def along(g, j, c, way, act):
        if way == 0:

            @pl.when(f > 0)
            def _():
                act(remote(g, j, r, c, 2 * n_rep, {"fs": f - 1}))

        else:

            @pl.when(f < n_fs - 1)
            def _():
                act(remote(g, j, r, c, 2 * n_rep + 1, {"fs": f + 1}))

    def start(copy):
        copy.start()

    def drain(copy):
        copy.wait_send()

    def onward(g, p, c, act):
        j = order(p)

        @pl.when(j > f)
        def _():
            along(g, j, c, 0, act)

        @pl.when(j < f)
        def _():
            along(g, j, c, 1, act)

        for d in range(1, n_rep):
            other = lax.rem(r + d, n_rep)
            act(remote(g, j, r, c, n_rep + other, {"rep": other}))

    def send_own(g):
        for c in range(chunk_counts[g]):
            along(g, f, c, 0, start)
            along(g, f, c, 1, start)

    def relay(g, p):
        for c in range(chunk_counts[g]):
            j = order(p)
            remote(g, j, r, c, 2 * n_rep, {"fs": f}).wait_recv()
            onward(g, p, c, start)

    def arrived(g, p):
        j = order(p)
        for d in range(1, n_rep):
            other = lax.rem(r + d, n_rep)
            for c in range(chunk_counts[g]):
                remote(g, j, other, c, n_rep + other, {"rep": other}).wait_recv()

    def block_of(index):
        return pl.ds(pl.multiple_of(index * rows, rows), rows)

    def copy_to(source, target, send_sem, recv_sem, device):
        return pltpu.make_async_remote_copy(
            src_ref=source,
            dst_ref=target,
            send_sem=send_sem,
            recv_sem=recv_sem,
            device_id=device,
            device_id_type=MESH,
        )

    def spread_rows(g, q, c):
        size = spread[g][0].shape[2] // n_rep // spread_counts[g]
        return pl.ds(pl.multiple_of((q * spread_counts[g] + c) * size, size), size)

    farthest = list(range(n_fs - 1, 0, -1))
    at_end = jnp.logical_or(f == 0, f == n_fs - 1)

    def by_place(ends, k):
        return jnp.where(at_end, order(ends[k - 1]), order(farthest[k - 1]))

    def ranked(k):
        return order(farthest[k - 1])

    far_steps = [(p, s) for p in range(n_fs - 1, 2, -1) for s in range(subs)]
    near_steps = [(1, s) for s in range(subs)]
    next_steps = [(2, s) for s in range(subs)]
    early = max(1, subs // 2)
    end_steps = next_steps[:early] + far_steps + near_steps + next_steps[early:]
    inner_steps = next_steps + far_steps + near_steps

    def step_of(k):
        if k < subs:
            return f, k
        (p, s), (q, u) = end_steps[k - subs], inner_steps[k - subs]
        return jnp.where(at_end, order(p), order(q)), jnp.where(at_end, s, u)

    def sent(k):
        return by_place(farthest[1:2] + farthest[:1] + farthest[2:], k)

    def spread_to(g, to, keep=lambda s, c: True):
        buf, arrivals, _, sent_sems = spread[g]
        slot = jnp.where(lax.rem(to, 2) == half, f, n_fs)
        for s in range(buf.shape[1]):
            for c in range(spread_counts[g]):
                if keep(s, c):
                    piece = spread_rows(g, r, c)
                    copy_to(
                        buf.at[slot, s, piece, :],
                        buf.at[f, s, piece, :],
                        sent_sems.at[n_rep],
                        arrivals.at[f, s, c],
                        {"fs": to},
                    ).start()

    def spread_own(g, keep=lambda k, c: True):
        for k in range(1, n_fs):
            spread_to(g, sent(k), lambda s, c: keep(k, c))

    def spread_late(g):
        def opening(s, c):
            return s == 0 and c == 0

        def rest(s, c):
            return not opening(s, c)

        @pl.when(at_end)
        def _():
            spread_to(g, order(1))
            for p in range(n_fs - 1, 1, -1):
                spread_to(g, order(p))

        @pl.when(jnp.logical_not(at_end))
        def _():
            spread_to(g, order(1), opening)
            for p in range(n_fs - 1, 2, -1):
                spread_to(g, order(p))
            spread_to(g, order(1), rest)
            spread_to(g, order(2))

    def spread_relay(g, j, s, chunks=None):
        buf, arrivals, swaps, sent_sems = spread[g]
        for c in range(spread_counts[g]) if chunks is None else chunks:
            block = buf.at[j, s, spread_rows(g, r, c), :]
            copy_to(block, block, sent_sems.at[n_rep], arrivals.at[j, s, c], {"fs": j}).wait_recv()
            for e in range(1, n_rep):
                other = lax.rem(r + e, n_rep)
                copy_to(
                    block, block, sent_sems.at[other], swaps.at[r, j, s], {"rep": other}
                ).start()

    def share_of(g, q):
        size = spread[g][0].shape[2] // n_rep
        return pl.ds(pl.multiple_of(q * size, size), size)

    def spread_arrived(g, j, s):
        buf, _, swaps, sent_sems = spread[g]
        for e in range(1, n_rep):
            other = lax.rem(r + e, n_rep)
            block = buf.at[j, s, share_of(g, other), :]
            copy_to(
                block, block, sent_sems.at[other], swaps.at[other, j, s], {"rep": other}
            ).wait_recv()

    def spread_drain(g):
        buf, arrivals, _, sent_sems = spread[g]
        block = buf.at[: n_fs - 1, :, share_of(g, 0), :]
        for e in range(1, n_rep):
            other = lax.rem(r + e, n_rep)
            copy_to(
                block, block, sent_sems.at[other], arrivals.at[0, 0, 0], {"rep": other}
            ).wait_send()
        copy_to(
            block, block, sent_sems.at[n_rep], arrivals.at[0, 0, 0], {"tp": t_pair}
        ).wait_send()

    def drained(block, sem):
        copy_to(block, block, sem, sem, {"tp": t_pair}).wait_send()

    stream = tokens[...].astype(jnp.float32)
    scale = lax.rsqrt(jnp.mean(stream * stream, axis=-1, keepdims=True) + epsilon)
    normed[block_of(t), :] = (stream * scale * gain1[...]).astype(jnp.bfloat16)

    def on_line(e):
        return lax.rem(y + e, n_y)

    def give_normed(owner, slot, device):
        block = normed.at[block_of(owner), :]
        return copy_to(block, block, normed_send.at[slot], normed_recv.at[owner], device)

    def normed_from(owner):
        give_normed(owner, 1, {"tp": t_pair}).wait_recv()

    pl.semaphore_wait(barrier, len(greeted))
    for e in range(1, n_y):
        to = on_line(e)
        give_normed(t, 0, {"tp": 2 * to + core}).start()
    give_normed(t, 1, {"tp": t_pair}).start()
    loads[0].wait()
    send_own(0)
    loads[1].wait()
    send_own(1)
    for p in range(1, n_fs):
        relay(0, p)
    for p in range(1, n_fs):
        relay(1, p)
    for e in range(1, n_y):
        owner = 2 * on_line(e) + core
        normed_from(owner)
        give_normed(owner, 1, {"tp": t_pair}).start()
    for copy in loads[2:]:
        copy.wait()

    def first_part(k, c):
        return k == 2 and c < spread_counts[0] // 2

    @pl.when(at_end)
    def _():
        spread_own(0)

    @pl.when(jnp.logical_not(at_end))
    def _():
        spread_own(0, first_part)

    for p in range(1, n_fs):
        arrived(0, p)
    for e in range(n_y):
        normed_from(2 * on_line(e) + 1 - core)
    total = dot(normed[:, :part], in_buf[0])
    for index in range(1, n_fs):
        total += dot(normed[:, index * part : (index + 1) * part], in_buf[index])
    projected[...] = total.astype(jnp.bfloat16).astype(jnp.float32)
    groups, channels = group_weight.shape[0], group_weight.shape[1]
    position = lax.broadcasted_iota(jnp.int32, (length, channels), 0)
    for group in range(groups):
        lanes = slice(group * channels, (group + 1) * channels)
        values = projected[:, lanes]
        level_of = jnp.full((length, channels), lax.rem(t * groups + group, LEVELS), jnp.int32)
        running = values
        mean = jnp.zeros_like(values)
        for level in range(LEVELS):
            offset = 2**level
            running = running + jnp.where(position >= offset, pltpu.roll(running, offset, 0), 0.0)
            count = jnp.minimum(position + 1, 2 * offset).astype(jnp.float32)
            mean = jnp.where(level_of == level, running / count, mean)
        pooled = (mean - values).astype(jnp.bfloat16)
        mapped = dot(pooled, group_weight[group])
        pool_out[:, lanes] = (mapped * pool_scale[:, lanes]).astype(jnp.bfloat16)

    @pl.when(jnp.logical_not(at_end))
    def _():
        spread_own(0, lambda k, c: not first_part(k, c))

    for p in range(1, n_fs):
        arrived(1, p)

    def mix_by_core(index, e):
        block = mix_send.at[index, block_of(2 * e + 1 - core), :]
        return copy_to(
            block, mix_core.at[index, e], mix_sent.at[0], mix_core_sems.at[index], {"tp": t_pair}
        )

    def mix_by_line(index, source, target, e, to):
        return copy_to(
            source, target, mix_sent.at[1], mix_line_sems.at[index, e], {"tp": 2 * to + core}
        )

    def mix_pair(index, which):
        own = mix_send[index, block_of(2 * which + core), :].astype(jnp.float32)
        return own + mix_core[index, which].astype(jnp.float32)

    for index in range(n_fs):
        mix_send[index] = dot(pool_out[...], out_buf[index]).astype(jnp.bfloat16)
        for e in range(n_y):
            mix_by_core(index, e).start()
    for index in range(n_fs):
        block = mix_core.at[index]
        copy_to(block, block, mix_sent.at[0], mix_core_sems.at[index], {"tp": t_pair}).wait_recv()
        for e in range(1, n_y):
            to = on_line(e)
            mix_line_send[index, to] = mix_pair(index, to).astype(jnp.bfloat16)
            source, target = mix_line_send.at[index, to], mix_line.at[index, y]
            mix_by_line(index, source, target, n_y - e - 1, to).start()

    @pl.when(jnp.logical_not(at_end))
    def _():
        spread_relay(0, ranked(1), 0)

    square = jnp.zeros((rows, 1), jnp.float32)
    for index in range(n_fs):
        mixed = tokens[:, index * part : (index + 1) * part].astype(jnp.float32)
        mixed += mix_pair(index, y)
        for e in range(1, n_y):
            block = mix_line.at[index, on_line(e)]
            mix_by_line(index, block, block, e - 1, on_line(e)).wait_recv()
            mixed += block[...].astype(jnp.float32)
        stream2[index] = mixed
        square += jnp.sum(mixed * mixed, axis=-1, keepdims=True)
    scale = lax.rsqrt(square / width + epsilon)

    def place_of(owner):
        return block_of(lax.rem(owner, 2) * n_y + owner // 2)

    for index in range(n_fs):
        columns = slice(index * part, (index + 1) * part)
        shared[half, place_of(t), columns] = (stream2[index] * scale * gain2[:, columns]).astype(
            jnp.bfloat16
        )

    def share(plane, owner, c, sent_sem, sem, device):
        size = rows // SHARE_CHUNKS
        place = lax.rem(owner, 2) * n_y + owner // 2
        start = pl.multiple_of(place * rows + c * size, size)
        block = shared.at[plane, pl.ds(start, size), :]
        return copy_to(block, block, share_sent.at[sent_sem], sem, device)

    def share_core(plane, owner, c):
        share(plane, owner, c, 0, share_core_sems.at[plane], {"tp": t_pair}).start()

    def by_line(plane, owner, c, e, to):
        sem = share_line_sems.at[plane, e, c]
        return share(plane, owner, c, 1, sem, {"tp": 2 * to + core})

    def share_line(plane, c):
        for e in range(1, n_y):
            by_line(plane, t, c, n_y - e - 1, on_line(e)).start()

    def pass_line(plane, c):
        for e in range(1, n_y):
            owner = 2 * on_line(e) + core
            by_line(plane, owner, c, e - 1, on_line(e)).wait_recv()
            share_core(plane, owner, c)

    def by_pair(plane, c):
        return share(plane, t, c, 2, share_pair_sems.at[c], {"fs": f_pair})

    def shared_by_core(plane):
        block = shared.at[plane, block_rows(1 - core), :]
        copy_to(
            block, block, share_sent.at[0], share_core_sems.at[plane], {"tp": t_pair}
        ).wait_recv()

    line_rows = n_y * rows

    def block_rows(which):
        return pl.ds(pl.multiple_of(which * line_rows, line_rows), line_rows)

    for c in range(SHARE_CHUNKS):
        by_pair(half, c).start()
        share_line(half, c)
        share_core(half, t, c)
    spread_late(1)

    @pl.when(at_end)
    def _():
        spread_relay(0, ranked(1), 0)

    for c in range(SHARE_CHUNKS):
        pass_line(half, c)
    for k in range(2, n_fs - 1):
        spread_relay(0, ranked(k), 0)

    @pl.when(at_end)
    def _():
        spread_relay(0, ranked(n_fs - 1), 0)

    last_chunks = spread_counts[0]
    for c in range(SHARE_CHUNKS):
        by_pair(1 - half, c).wait_recv()
        share_line(1 - half, c)
        share_core(1 - half, t, c)
        begin, end = c * last_chunks // SHARE_CHUNKS, (c + 1) * last_chunks // SHARE_CHUNKS

        @pl.when(jnp.logical_not(at_end))
        def _():
            spread_relay(0, ranked(n_fs - 1), 0, range(begin, end))

    for c in range(SHARE_CHUNKS):
        pass_line(1 - half, c)
    shared_by_core(half)
    for d in range(1, n_fs):
        spread_arrived(0, ranked(d), 0)

    up_tile = tile_of(half_units, 256)

    def up_product(plane):
        @pl.loop(0, half_units // up_tile)
        def _(i):
            columns = pl.ds(pl.multiple_of(i * up_tile, up_tile), up_tile)
            total = dot(shared[plane, :, :part], up_buf[0, 0, :, columns])
            for index in range(1, n_fs):
                left = shared[plane, :, index * part : (index + 1) * part]
                total += dot(left, up_buf[index, 0, :, columns])
            value = jnp.maximum(total, 0.0)
            hidden[plane, :, columns] = (value * value).astype(jnp.bfloat16)

    relayed = [subs]

    def relay_steps(upto):
        while relayed[0] < min(upto, steps):
            j, s = step_of(relayed[0])
            relayed[0] += 1
            spread_relay(1, j, s)

    relay_steps(subs + subs // 2)
    up_product(half)
    relay_steps(2 * subs - 1)
    shared_by_core(1 - half)
    up_product(1 - half)

    def columns_of(s):
        return pl.ds(pl.multiple_of(s * sub_columns, sub_columns), sub_columns)

    def down_product(k):
        j, s = step_of(k)
        if k >= subs:
            spread_arrived(1, j, s)
        for plane in range(2):
            product = dot(hidden[plane], down_buf[j, s])
            core_send[k, plane] = product.astype(jnp.bfloat16)
        copy_to(
            core_send.at[k, :, block_rows(1 - core), :],
            core_recv.at[k],
            sums_sent.at[0],
            core_sems.at[k],
            {"tp": t_pair},
        ).start()

    def to_line(k):
        block = core_recv.at[k]
        copy_to(block, block, sums_sent.at[0], core_sems.at[k], {"tp": t_pair}).wait_recv()
        for plane in range(2):
            own = core_send[k, plane, block_rows(core), :].astype(jnp.float32)
            both = own + core_recv[k, plane].astype(jnp.float32)
            line_send[k, plane] = both.astype(jnp.bfloat16)
        for e in range(1, n_y):
            to = on_line(e)
            copy_to(
                line_send.at[k, :, block_of(to), :],
                line_recv.at[k, y],
                sums_sent.at[1],
                line_sems.at[k, n_y - e - 1],
                {"tp": 2 * to + core},
            ).start()

    def to_pair(k):
        j, s = step_of(k)
        for e in range(1, n_y):
            block = line_recv.at[k, on_line(e)]
            copy_to(
                block, block, sums_sent.at[1], line_sems.at[k, e - 1], {"tp": t_pair}
            ).wait_recv()

        def total_of(plane):
            total = core_send[k, plane, block_of(core * n_y + y), :].astype(jnp.float32)
            total += core_recv[k, plane, block_of(y), :].astype(jnp.float32)
            for e in range(1, n_y):
                total += line_recv[k, on_line(e), plane].astype(jnp.float32)
            return total

        pair_send[j * subs + s] = total_of(1 - half).astype(jnp.bfloat16)
        slot = j * subs + s
        copy_to(
            pair_send.at[slot],
            pair_recv.at[slot],
            sums_sent.at[2],
            pair_sems.at[slot],
            {"fs": f_pair},
        ).start()
        columns = columns_of(s)
        stream2[j, :, columns] += total_of(half)

    def finish(k):
        j, s = step_of(k)
        slot = j * subs + s
        block = pair_recv.at[slot]
        copy_to(block, block, sums_sent.at[2], pair_sems.at[slot], {"fs": f_pair}).wait_recv()
        columns = columns_of(s)
        value = stream2[j, :, columns] + pair_recv[slot].astype(jnp.float32)
        target = pl.ds(pl.multiple_of(j * part + s * sub_columns, sub_columns), sub_columns)
        result[:, target] = value.astype(jnp.bfloat16)

    for k in range(steps + 4):
        relay_steps(k + AHEAD + 1)
        if k < steps:
            down_product(k)
        if 0 <= k - 1 < steps:
            to_line(k - 1)
        if 0 <= k - 4 < steps:
            to_pair(k - 4)
    for g in range(2):
        spread_drain(g)
        for c in range(chunk_counts[g]):
            along(g, f, c, 0, drain)
            along(g, f, c, 1, drain)
            for p in range(1, n_fs):
                onward(g, p, c, drain)
    drained(normed.at[: line_rows - rows, :], normed_send.at[0])
    drained(normed.at[:line_rows, :], normed_send.at[1])
    drained(mix_core, mix_sent.at[0])
    drained(mix_line.at[:, : n_y - 1], mix_sent.at[1])
    drained(shared.at[:, :line_rows, :], share_sent.at[0])
    drained(shared.at[:, : line_rows - rows, :], share_sent.at[1])
    drained(shared.at[0, :rows, :], share_sent.at[2])
    drained(core_recv, sums_sent.at[0])
    drained(line_recv.at[:, : n_y - 1], sums_sent.at[1])
    for k in range(steps):
        finish(k)
    drained(pair_recv, sums_sent.at[2])


def local(sizes, tokens, gain1, in_w, group_w, pool_scale, out_w, gain2, up_w, down_w):
    n_rep, n_fs, n_tp = sizes
    n_y = n_tp // 2
    rows, width = tokens.shape
    length, part = rows * n_tp, width // n_fs
    channels, half_units = in_w.shape[1], up_w.shape[1] // 2
    sub_columns = tile_of(part, SUB_COLUMNS)
    subs = part // sub_columns
    steps = n_fs * subs
    bf16, f32 = jnp.bfloat16, jnp.float32
    vmem = pl.BlockSpec(memory_space=pltpu.VMEM)
    hbm = pl.BlockSpec(memory_space=pl.ANY)
    dma = pltpu.SemaphoreType.DMA
    return pl.pallas_call(
        functools.partial(kernel, sizes),
        name="layer",
        out_shape=jax.ShapeDtypeStruct((rows, width), bf16),
        in_specs=[vmem, vmem, hbm, vmem, vmem, hbm, vmem, hbm, hbm],
        out_specs=vmem,
        scratch_shapes=[
            pltpu.VMEM((n_fs,) + in_w.shape, bf16),
            pltpu.VMEM((n_fs,) + out_w.shape, bf16),
            pltpu.VMEM((n_fs + 1, 1, part, half_units), bf16),
            pltpu.VMEM((n_fs + 1, subs, half_units, sub_columns), bf16),
            pltpu.VMEM((length, width), bf16),
            pltpu.VMEM((length, channels), f32),
            pltpu.VMEM((length, channels), bf16),
            pltpu.VMEM((n_fs, length, part), bf16),
            pltpu.VMEM((n_fs, n_y, rows, part), bf16),
            pltpu.VMEM((n_fs, n_y, rows, part), bf16),
            pltpu.VMEM((n_fs, n_y, rows, part), bf16),
            pltpu.VMEM((n_fs, rows, part), f32),
            pltpu.VMEM((2, length, width), bf16),
            pltpu.VMEM((2, length, half_units), bf16),
            pltpu.VMEM((steps, 2, length, sub_columns), bf16),
            pltpu.VMEM((steps, 2, n_y * rows, sub_columns), bf16),
            pltpu.VMEM((steps, 2, n_y * rows, sub_columns), bf16),
            pltpu.VMEM((steps, n_y, 2, rows, sub_columns), bf16),
            pltpu.VMEM((steps, rows, sub_columns), bf16),
            pltpu.VMEM((steps, rows, sub_columns), bf16),
            dma((4 + 2 * subs,)),
            dma((n_fs, 2 * n_rep + 2, chunks_of(*in_w.shape, n_rep))),
            dma((n_fs, 2 * n_rep + 2, chunks_of(*out_w.shape, n_rep))),
            dma((n_fs, 1, chunks_of(part, half_units, n_rep))),
            dma((n_rep, n_fs, 1)),
            dma((n_rep + 1,)),
            dma((n_fs, subs, chunks_of(half_units, sub_columns, n_rep))),
            dma((n_rep, n_fs, subs)),
            dma((n_rep + 1,)),
            dma((2,)),
            dma((n_tp,)),
            dma((2,)),
            dma((n_fs,)),
            dma((n_fs, n_y - 1)),
            dma((3,)),
            dma((2,)),
            dma((2, n_y - 1, SHARE_CHUNKS)),
            dma((SHARE_CHUNKS,)),
            dma((3,)),
            dma((steps,)),
            dma((steps, n_y - 1)),
            dma((steps,)),
        ],
        compiler_params=pltpu.CompilerParams(
            collective_id=0, has_side_effects=True, vmem_limit_bytes=60 * 1024 * 1024
        ),
    )(
        tokens,
        gain1.reshape(1, -1),
        in_w,
        group_w,
        pool_scale.reshape(1, -1),
        out_w,
        gain2.reshape(1, -1),
        up_w,
        down_w,
    )


def solution(mesh):
    sizes = tuple(mesh.shape[axis] for axis in ("rep", "fs", "tp"))
    in_specs = (
        P(("rep", "fs", "tp"), None),
        P(),
        P("fs", "tp"),
        P("tp", None, None),
        P("tp"),
        P("tp", "fs"),
        P(),
        P("fs", "tp"),
        P("tp", "fs"),
    )
    return jax.shard_map(
        functools.partial(local, sizes),
        mesh=mesh,
        in_specs=in_specs,
        out_specs=P(("rep", "fs", "tp"), None),
        check_vma=False,
    )
```

```python
import functools

import jax
import jax.numpy as jnp
from jax import lax
from jax.experimental import pallas as pl
from jax.experimental.pallas import tpu as pltpu
from jax.sharding import PartitionSpec as P

MESH = pl.DeviceIdType.MESH
CHUNK_BYTES = 128 * 1024
SUB_COLUMNS = 256
AHEAD = 2
SHARE_CHUNKS = 4
LEVELS = 4

epsilon = 1e-06


def chunks_of(rows, columns, parts):
    count = max(1, rows * columns * 2 // parts // CHUNK_BYTES)
    while (rows // parts) % (count * 16):
        count -= 1
    return count


def dot(a, b):
    return jnp.dot(a, b, preferred_element_type=jnp.float32)


def tile_of(columns, most):
    tile = min(columns, most)
    while columns % tile:
        tile //= 2
    return tile


def kernel(
    sizes,
    tokens,
    gain1,
    in_hbm,
    group_weight,
    pool_scale,
    out_hbm,
    gain2,
    up_hbm,
    down_hbm,
    result,
    in_buf,
    out_buf,
    up_buf,
    down_buf,
    normed,
    projected,
    pool_out,
    mix_send,
    mix_core,
    mix_line_send,
    mix_line,
    stream2,
    shared,
    hidden,
    core_send,
    core_recv,
    line_send,
    line_recv,
    pair_send,
    pair_recv,
    local_sem,
    in_sems,
    out_sems,
    up_arrivals,
    up_swaps,
    up_sent,
    down_arrivals,
    down_swaps,
    down_sent,
    normed_send,
    normed_recv,
    mix_sent,
    mix_core_sems,
    mix_line_sems,
    share_sent,
    share_core_sems,
    share_line_sems,
    share_pair_sems,
    sums_sent,
    core_sems,
    line_sems,
    pair_sems,
):
    n_rep, n_fs, n_tp = sizes
    n_y = n_tp // 2
    r, f, t = lax.axis_index("rep"), lax.axis_index("fs"), lax.axis_index("tp")
    core, y = lax.rem(t, 2), t // 2
    half = lax.rem(f, 2)
    f_pair, t_pair = f + 1 - 2 * half, t + 1 - 2 * core
    rows = tokens.shape[0]
    length = rows * n_tp
    width = tokens.shape[1]
    part = width // n_fs
    subs = down_buf.shape[1]
    sub_columns = down_buf.shape[3]
    steps = n_fs * subs
    half_units = up_buf.shape[3]
    gathered = ((in_buf, in_sems), (out_buf, out_sems))
    chunk_counts = [chunks_of(b.shape[1], b.shape[2], n_rep) for b, _ in gathered]
    spread = (
        (up_buf, up_arrivals, up_swaps, up_sent),
        (down_buf, down_arrivals, down_swaps, down_sent),
    )
    spread_counts = [chunks_of(item[0].shape[2], item[0].shape[3], n_rep) for item in spread]

    loads = []

    def load(source, target):
        copy = pltpu.make_async_copy(source, target, local_sem.at[len(loads)])
        copy.start()
        loads.append(copy)

    def units_of(which):
        return pl.ds(pl.multiple_of(which * half_units, half_units), half_units)

    load(in_hbm, in_buf.at[f])
    load(out_hbm, out_buf.at[f])
    load(up_hbm.at[:, units_of(1 - half)], up_buf.at[n_fs, 0])
    load(up_hbm.at[:, units_of(half)], up_buf.at[f, 0])
    for s in range(subs):
        columns = pl.ds(s * sub_columns, sub_columns)
        load(down_hbm.at[units_of(1 - half), columns], down_buf.at[n_fs, s])
        load(down_hbm.at[units_of(half), columns], down_buf.at[f, s])

    barrier = pltpu.get_barrier_semaphore()
    greeted = [{"fs": lax.rem(f + d, n_fs)} for d in range(1, n_fs)]
    greeted += [{"rep": lax.rem(r + d, n_rep)} for d in range(1, n_rep)]
    greeted += [{"tp": lax.rem(t + d, n_tp)} for d in range(1, n_tp)]
    for device in greeted:
        pl.semaphore_signal(barrier, inc=1, device_id=device, device_id_type=MESH)

    inward = jnp.where(2 * f < n_fs, 1, -1)

    def order(p):
        nearest = jnp.minimum(f, n_fs - 1 - f)
        step = (p + 1) // 2
        near = f + step * inward if p % 2 else f - step * inward
        far = f + (p - nearest) * inward
        return jnp.where(p <= 2 * nearest, near, far)

    def piece(g, j, q, c):
        buf = gathered[g][0]
        size = buf.shape[1] // n_rep // chunk_counts[g]
        start = pl.multiple_of((q * chunk_counts[g] + c) * size, size)
        return buf.at[j, pl.ds(start, size), :]

    def remote(g, j, q, c, send_slot, device):
        block = piece(g, j, q, c)
        sems = gathered[g][1]
        return pltpu.make_async_remote_copy(
            src_ref=block,
            dst_ref=block,
            send_sem=sems.at[j, send_slot, c],
            recv_sem=sems.at[j, q, c],
            device_id=device,
            device_id_type=MESH,
        )

    def along(g, j, c, way, act):
        if way == 0:

            @pl.when(f > 0)
            def _():
                act(remote(g, j, r, c, 2 * n_rep, {"fs": f - 1}))

        else:

            @pl.when(f < n_fs - 1)
            def _():
                act(remote(g, j, r, c, 2 * n_rep + 1, {"fs": f + 1}))

    def start(copy):
        copy.start()

    def drain(copy):
        copy.wait_send()

    def onward(g, p, c, act):
        j = order(p)

        @pl.when(j > f)
        def _():
            along(g, j, c, 0, act)

        @pl.when(j < f)
        def _():
            along(g, j, c, 1, act)

        for d in range(1, n_rep):
            other = lax.rem(r + d, n_rep)
            act(remote(g, j, r, c, n_rep + other, {"rep": other}))

    def send_own(g):
        for c in range(chunk_counts[g]):
            along(g, f, c, 0, start)
            along(g, f, c, 1, start)

    def relay(g, p):
        for c in range(chunk_counts[g]):
            j = order(p)
            remote(g, j, r, c, 2 * n_rep, {"fs": f}).wait_recv()
            onward(g, p, c, start)

    def arrived(g, p):
        j = order(p)
        for d in range(1, n_rep):
            other = lax.rem(r + d, n_rep)
            for c in range(chunk_counts[g]):
                remote(g, j, other, c, n_rep + other, {"rep": other}).wait_recv()

    def block_of(index):
        return pl.ds(pl.multiple_of(index * rows, rows), rows)

    def copy_to(source, target, send_sem, recv_sem, device):
        return pltpu.make_async_remote_copy(
            src_ref=source,
            dst_ref=target,
            send_sem=send_sem,
            recv_sem=recv_sem,
            device_id=device,
            device_id_type=MESH,
        )

    def spread_rows(g, q, c):
        size = spread[g][0].shape[2] // n_rep // spread_counts[g]
        return pl.ds(pl.multiple_of((q * spread_counts[g] + c) * size, size), size)

    farthest = list(range(n_fs - 1, 0, -1))
    at_end = jnp.logical_or(f == 0, f == n_fs - 1)

    def by_place(ends, k):
        return jnp.where(at_end, order(ends[k - 1]), order(farthest[k - 1]))

    def ranked(k):
        return order(farthest[k - 1])

    far_steps = [(p, s) for p in range(n_fs - 1, 2, -1) for s in range(subs)]
    near_steps = [(1, s) for s in range(subs)]
    next_steps = [(2, s) for s in range(subs)]
    early = max(1, subs // 2)
    end_steps = next_steps[:early] + far_steps + near_steps + next_steps[early:]
    inner_steps = next_steps + far_steps + near_steps

    def step_of(k):
        if k < subs:
            return f, k
        (p, s), (q, u) = end_steps[k - subs], inner_steps[k - subs]
        return jnp.where(at_end, order(p), order(q)), jnp.where(at_end, s, u)

    def sent(k):
        return by_place(farthest[1:2] + farthest[:1] + farthest[2:], k)

    def spread_to(g, to, keep=lambda s, c: True):
        buf, arrivals, _, sent_sems = spread[g]
        slot = jnp.where(lax.rem(to, 2) == half, f, n_fs)
        for s in range(buf.shape[1]):
            for c in range(spread_counts[g]):
                if keep(s, c):
                    piece = spread_rows(g, r, c)
                    copy_to(
                        buf.at[slot, s, piece, :],
                        buf.at[f, s, piece, :],
                        sent_sems.at[n_rep],
                        arrivals.at[f, s, c],
                        {"fs": to},
                    ).start()

    def spread_own(g, keep=lambda k, c: True):
        for k in range(1, n_fs):
            spread_to(g, sent(k), lambda s, c: keep(k, c))

    def spread_late(g):
        def opening(s, c):
            return s == 0 and c == 0

        def rest(s, c):
            return not opening(s, c)

        @pl.when(at_end)
        def _():
            spread_to(g, order(1))
            for p in range(n_fs - 1, 1, -1):
                spread_to(g, order(p))

        @pl.when(jnp.logical_not(at_end))
        def _():
            spread_to(g, order(1), opening)
            for p in range(n_fs - 1, 2, -1):
                spread_to(g, order(p))
            spread_to(g, order(1), rest)
            spread_to(g, order(2))

    def spread_relay(g, j, s, chunks=None):
        buf, arrivals, swaps, sent_sems = spread[g]
        for c in range(spread_counts[g]) if chunks is None else chunks:
            block = buf.at[j, s, spread_rows(g, r, c), :]
            copy_to(block, block, sent_sems.at[n_rep], arrivals.at[j, s, c], {"fs": j}).wait_recv()
            for e in range(1, n_rep):
                other = lax.rem(r + e, n_rep)
                copy_to(
                    block, block, sent_sems.at[other], swaps.at[r, j, s], {"rep": other}
                ).start()

    def share_of(g, q):
        size = spread[g][0].shape[2] // n_rep
        return pl.ds(pl.multiple_of(q * size, size), size)

    def spread_arrived(g, j, s):
        buf, _, swaps, sent_sems = spread[g]
        for e in range(1, n_rep):
            other = lax.rem(r + e, n_rep)
            block = buf.at[j, s, share_of(g, other), :]
            copy_to(
                block, block, sent_sems.at[other], swaps.at[other, j, s], {"rep": other}
            ).wait_recv()

    def spread_drain(g):
        buf, arrivals, _, sent_sems = spread[g]
        block = buf.at[: n_fs - 1, :, share_of(g, 0), :]
        for e in range(1, n_rep):
            other = lax.rem(r + e, n_rep)
            copy_to(
                block, block, sent_sems.at[other], arrivals.at[0, 0, 0], {"rep": other}
            ).wait_send()
        copy_to(
            block, block, sent_sems.at[n_rep], arrivals.at[0, 0, 0], {"tp": t_pair}
        ).wait_send()

    def drained(block, sem):
        copy_to(block, block, sem, sem, {"tp": t_pair}).wait_send()

    stream = tokens[...].astype(jnp.float32)
    scale = lax.rsqrt(jnp.mean(stream * stream, axis=-1, keepdims=True) + epsilon)
    normed[block_of(t), :] = (stream * scale * gain1[...]).astype(jnp.bfloat16)

    def on_line(e):
        return lax.rem(y + e, n_y)

    def give_normed(owner, slot, device):
        block = normed.at[block_of(owner), :]
        return copy_to(block, block, normed_send.at[slot], normed_recv.at[owner], device)

    def normed_from(owner):
        give_normed(owner, 1, {"tp": t_pair}).wait_recv()

    pl.semaphore_wait(barrier, len(greeted))
    for e in range(1, n_y):
        to = on_line(e)
        give_normed(t, 0, {"tp": 2 * to + core}).start()
    give_normed(t, 1, {"tp": t_pair}).start()
    loads[0].wait()
    send_own(0)
    loads[1].wait()
    send_own(1)
    for p in range(1, n_fs):
        relay(0, p)
    for p in range(1, n_fs):
        relay(1, p)
    for e in range(1, n_y):
        owner = 2 * on_line(e) + core
        normed_from(owner)
        give_normed(owner, 1, {"tp": t_pair}).start()
    for copy in loads[2:]:
        copy.wait()

    def first_part(k, c):
        return k == 2 and c < spread_counts[0] // 2

    @pl.when(at_end)
    def _():
        spread_own(0)

    @pl.when(jnp.logical_not(at_end))
    def _():
        spread_own(0, first_part)

    for p in range(1, n_fs):
        arrived(0, p)
    for e in range(n_y):
        normed_from(2 * on_line(e) + 1 - core)
    total = dot(normed[:, :part], in_buf[0])
    for index in range(1, n_fs):
        total += dot(normed[:, index * part : (index + 1) * part], in_buf[index])
    projected[...] = total.astype(jnp.bfloat16).astype(jnp.float32)
    groups, channels = group_weight.shape[0], group_weight.shape[1]
    position = lax.broadcasted_iota(jnp.int32, (length, channels), 0)
    for group in range(groups):
        lanes = slice(group * channels, (group + 1) * channels)
        values = projected[:, lanes]
        level_of = jnp.full((length, channels), lax.rem(t * groups + group, LEVELS), jnp.int32)
        running = values
        mean = jnp.zeros_like(values)
        for level in range(LEVELS):
            offset = 2**level
            running = running + jnp.where(position >= offset, pltpu.roll(running, offset, 0), 0.0)
            count = jnp.minimum(position + 1, 2 * offset).astype(jnp.float32)
            mean = jnp.where(level_of == level, running / count, mean)
        pooled = (mean - values).astype(jnp.bfloat16)
        mapped = dot(pooled, group_weight[group])
        pool_out[:, lanes] = (mapped * pool_scale[:, lanes]).astype(jnp.bfloat16)

    @pl.when(jnp.logical_not(at_end))
    def _():
        spread_own(0, lambda k, c: not first_part(k, c))

    for p in range(1, n_fs):
        arrived(1, p)

    def mix_by_core(index, e):
        block = mix_send.at[index, block_of(2 * e + 1 - core), :]
        return copy_to(
            block, mix_core.at[index, e], mix_sent.at[0], mix_core_sems.at[index], {"tp": t_pair}
        )

    def mix_by_line(index, source, target, e, to):
        return copy_to(
            source, target, mix_sent.at[1], mix_line_sems.at[index, e], {"tp": 2 * to + core}
        )

    def mix_pair(index, which):
        own = mix_send[index, block_of(2 * which + core), :].astype(jnp.float32)
        return own + mix_core[index, which].astype(jnp.float32)

    for index in range(n_fs):
        mix_send[index] = dot(pool_out[...], out_buf[index]).astype(jnp.bfloat16)
        for e in range(n_y):
            mix_by_core(index, e).start()
    for index in range(n_fs):
        block = mix_core.at[index]
        copy_to(block, block, mix_sent.at[0], mix_core_sems.at[index], {"tp": t_pair}).wait_recv()
        for e in range(1, n_y):
            to = on_line(e)
            mix_line_send[index, to] = mix_pair(index, to).astype(jnp.bfloat16)
            source, target = mix_line_send.at[index, to], mix_line.at[index, y]
            mix_by_line(index, source, target, n_y - e - 1, to).start()

    @pl.when(jnp.logical_not(at_end))
    def _():
        spread_relay(0, ranked(1), 0)

    square = jnp.zeros((rows, 1), jnp.float32)
    for index in range(n_fs):
        mixed = tokens[:, index * part : (index + 1) * part].astype(jnp.float32)
        mixed += mix_pair(index, y)
        for e in range(1, n_y):
            block = mix_line.at[index, on_line(e)]
            mix_by_line(index, block, block, e - 1, on_line(e)).wait_recv()
            mixed += block[...].astype(jnp.float32)
        stream2[index] = mixed
        square += jnp.sum(mixed * mixed, axis=-1, keepdims=True)
    scale = lax.rsqrt(square / width + epsilon)

    def place_of(owner):
        return block_of(lax.rem(owner, 2) * n_y + owner // 2)

    for index in range(n_fs):
        columns = slice(index * part, (index + 1) * part)
        shared[half, place_of(t), columns] = (stream2[index] * scale * gain2[:, columns]).astype(
            jnp.bfloat16
        )

    def share(plane, owner, c, sent_sem, sem, device):
        size = rows // SHARE_CHUNKS
        place = lax.rem(owner, 2) * n_y + owner // 2
        start = pl.multiple_of(place * rows + c * size, size)
        block = shared.at[plane, pl.ds(start, size), :]
        return copy_to(block, block, share_sent.at[sent_sem], sem, device)

    def share_core(plane, owner, c):
        share(plane, owner, c, 0, share_core_sems.at[plane], {"tp": t_pair}).start()

    def by_line(plane, owner, c, e, to):
        sem = share_line_sems.at[plane, e, c]
        return share(plane, owner, c, 1, sem, {"tp": 2 * to + core})

    def share_line(plane, c):
        for e in range(1, n_y):
            by_line(plane, t, c, n_y - e - 1, on_line(e)).start()

    def pass_line(plane, c):
        for e in range(1, n_y):
            owner = 2 * on_line(e) + core
            by_line(plane, owner, c, e - 1, on_line(e)).wait_recv()
            share_core(plane, owner, c)

    def by_pair(plane, c):
        return share(plane, t, c, 2, share_pair_sems.at[c], {"fs": f_pair})

    def shared_by_core(plane):
        block = shared.at[plane, block_rows(1 - core), :]
        copy_to(
            block, block, share_sent.at[0], share_core_sems.at[plane], {"tp": t_pair}
        ).wait_recv()

    line_rows = n_y * rows

    def block_rows(which):
        return pl.ds(pl.multiple_of(which * line_rows, line_rows), line_rows)

    for c in range(SHARE_CHUNKS):
        by_pair(half, c).start()
        share_line(half, c)
        share_core(half, t, c)
    spread_late(1)

    @pl.when(at_end)
    def _():
        spread_relay(0, ranked(1), 0)

    for c in range(SHARE_CHUNKS):
        pass_line(half, c)
    for k in range(2, n_fs - 1):
        spread_relay(0, ranked(k), 0)

    @pl.when(at_end)
    def _():
        spread_relay(0, ranked(n_fs - 1), 0)

    last_chunks = spread_counts[0]
    for c in range(SHARE_CHUNKS):
        by_pair(1 - half, c).wait_recv()
        share_line(1 - half, c)
        share_core(1 - half, t, c)
        begin, end = c * last_chunks // SHARE_CHUNKS, (c + 1) * last_chunks // SHARE_CHUNKS

        @pl.when(jnp.logical_not(at_end))
        def _():
            spread_relay(0, ranked(n_fs - 1), 0, range(begin, end))

    for c in range(SHARE_CHUNKS):
        pass_line(1 - half, c)
    shared_by_core(half)
    for d in range(1, n_fs):
        spread_arrived(0, ranked(d), 0)

    up_tile = tile_of(half_units, 256)

    def up_product(plane):
        @pl.loop(0, half_units // up_tile)
        def _(i):
            columns = pl.ds(pl.multiple_of(i * up_tile, up_tile), up_tile)
            total = dot(shared[plane, :, :part], up_buf[0, 0, :, columns])
            for index in range(1, n_fs):
                left = shared[plane, :, index * part : (index + 1) * part]
                total += dot(left, up_buf[index, 0, :, columns])
            value = jnp.maximum(total, 0.0)
            hidden[plane, :, columns] = (value * value).astype(jnp.bfloat16)

    relayed = [subs]

    def relay_steps(upto):
        while relayed[0] < min(upto, steps):
            j, s = step_of(relayed[0])
            relayed[0] += 1
            spread_relay(1, j, s)

    relay_steps(subs + subs // 2)
    up_product(half)
    relay_steps(2 * subs - 1)
    shared_by_core(1 - half)
    up_product(1 - half)

    def columns_of(s):
        return pl.ds(pl.multiple_of(s * sub_columns, sub_columns), sub_columns)

    def down_product(k):
        j, s = step_of(k)
        if k >= subs:
            spread_arrived(1, j, s)
        for plane in range(2):
            product = dot(hidden[plane], down_buf[j, s])
            core_send[k, plane] = product.astype(jnp.bfloat16)
        copy_to(
            core_send.at[k, :, block_rows(1 - core), :],
            core_recv.at[k],
            sums_sent.at[0],
            core_sems.at[k],
            {"tp": t_pair},
        ).start()

    def to_line(k):
        block = core_recv.at[k]
        copy_to(block, block, sums_sent.at[0], core_sems.at[k], {"tp": t_pair}).wait_recv()
        for plane in range(2):
            own = core_send[k, plane, block_rows(core), :].astype(jnp.float32)
            both = own + core_recv[k, plane].astype(jnp.float32)
            line_send[k, plane] = both.astype(jnp.bfloat16)
        for e in range(1, n_y):
            to = on_line(e)
            copy_to(
                line_send.at[k, :, block_of(to), :],
                line_recv.at[k, y],
                sums_sent.at[1],
                line_sems.at[k, n_y - e - 1],
                {"tp": 2 * to + core},
            ).start()

    def to_pair(k):
        j, s = step_of(k)
        for e in range(1, n_y):
            block = line_recv.at[k, on_line(e)]
            copy_to(
                block, block, sums_sent.at[1], line_sems.at[k, e - 1], {"tp": t_pair}
            ).wait_recv()

        def total_of(plane):
            total = core_send[k, plane, block_of(core * n_y + y), :].astype(jnp.float32)
            total += core_recv[k, plane, block_of(y), :].astype(jnp.float32)
            for e in range(1, n_y):
                total += line_recv[k, on_line(e), plane].astype(jnp.float32)
            return total

        pair_send[j * subs + s] = total_of(1 - half).astype(jnp.bfloat16)
        slot = j * subs + s
        copy_to(
            pair_send.at[slot],
            pair_recv.at[slot],
            sums_sent.at[2],
            pair_sems.at[slot],
            {"fs": f_pair},
        ).start()
        columns = columns_of(s)
        stream2[j, :, columns] += total_of(half)

    def finish(k):
        j, s = step_of(k)
        slot = j * subs + s
        block = pair_recv.at[slot]
        copy_to(block, block, sums_sent.at[2], pair_sems.at[slot], {"fs": f_pair}).wait_recv()
        columns = columns_of(s)
        value = stream2[j, :, columns] + pair_recv[slot].astype(jnp.float32)
        target = pl.ds(pl.multiple_of(j * part + s * sub_columns, sub_columns), sub_columns)
        result[:, target] = value.astype(jnp.bfloat16)

    for k in range(steps + 4):
        relay_steps(k + AHEAD + 1)
        if k < steps:
            down_product(k)
        if 0 <= k - 1 < steps:
            to_line(k - 1)
        if 0 <= k - 4 < steps:
            to_pair(k - 4)
    for g in range(2):
        spread_drain(g)
        for c in range(chunk_counts[g]):
            along(g, f, c, 0, drain)
            along(g, f, c, 1, drain)
            for p in range(1, n_fs):
                onward(g, p, c, drain)
    drained(normed.at[: line_rows - rows, :], normed_send.at[0])
    drained(normed.at[:line_rows, :], normed_send.at[1])
    drained(mix_core, mix_sent.at[0])
    drained(mix_line.at[:, : n_y - 1], mix_sent.at[1])
    drained(shared.at[:, :line_rows, :], share_sent.at[0])
    drained(shared.at[:, : line_rows - rows, :], share_sent.at[1])
    drained(shared.at[0, :rows, :], share_sent.at[2])
    drained(core_recv, sums_sent.at[0])
    drained(line_recv.at[:, : n_y - 1], sums_sent.at[1])
    for k in range(steps):
        finish(k)
    drained(pair_recv, sums_sent.at[2])


def local(sizes, tokens, gain1, in_w, group_w, pool_scale, out_w, gain2, up_w, down_w):
    n_rep, n_fs, n_tp = sizes
    n_y = n_tp // 2
    rows, width = tokens.shape
    length, part = rows * n_tp, width // n_fs
    channels, half_units = in_w.shape[1], up_w.shape[1] // 2
    sub_columns = tile_of(part, SUB_COLUMNS)
    subs = part // sub_columns
    steps = n_fs * subs
    bf16, f32 = jnp.bfloat16, jnp.float32
    vmem = pl.BlockSpec(memory_space=pltpu.VMEM)
    hbm = pl.BlockSpec(memory_space=pl.ANY)
    dma = pltpu.SemaphoreType.DMA
    return pl.pallas_call(
        functools.partial(kernel, sizes),
        name="layer",
        out_shape=jax.ShapeDtypeStruct((rows, width), bf16),
        in_specs=[vmem, vmem, hbm, vmem, vmem, hbm, vmem, hbm, hbm],
        out_specs=vmem,
        scratch_shapes=[
            pltpu.VMEM((n_fs,) + in_w.shape, bf16),
            pltpu.VMEM((n_fs,) + out_w.shape, bf16),
            pltpu.VMEM((n_fs + 1, 1, part, half_units), bf16),
            pltpu.VMEM((n_fs + 1, subs, half_units, sub_columns), bf16),
            pltpu.VMEM((length, width), bf16),
            pltpu.VMEM((length, channels), f32),
            pltpu.VMEM((length, channels), bf16),
            pltpu.VMEM((n_fs, length, part), bf16),
            pltpu.VMEM((n_fs, n_y, rows, part), bf16),
            pltpu.VMEM((n_fs, n_y, rows, part), bf16),
            pltpu.VMEM((n_fs, n_y, rows, part), bf16),
            pltpu.VMEM((n_fs, rows, part), f32),
            pltpu.VMEM((2, length, width), bf16),
            pltpu.VMEM((2, length, half_units), bf16),
            pltpu.VMEM((steps, 2, length, sub_columns), bf16),
            pltpu.VMEM((steps, 2, n_y * rows, sub_columns), bf16),
            pltpu.VMEM((steps, 2, n_y * rows, sub_columns), bf16),
            pltpu.VMEM((steps, n_y, 2, rows, sub_columns), bf16),
            pltpu.VMEM((steps, rows, sub_columns), bf16),
            pltpu.VMEM((steps, rows, sub_columns), bf16),
            dma((4 + 2 * subs,)),
            dma((n_fs, 2 * n_rep + 2, chunks_of(*in_w.shape, n_rep))),
            dma((n_fs, 2 * n_rep + 2, chunks_of(*out_w.shape, n_rep))),
            dma((n_fs, 1, chunks_of(part, half_units, n_rep))),
            dma((n_rep, n_fs, 1)),
            dma((n_rep + 1,)),
            dma((n_fs, subs, chunks_of(half_units, sub_columns, n_rep))),
            dma((n_rep, n_fs, subs)),
            dma((n_rep + 1,)),
            dma((2,)),
            dma((n_tp,)),
            dma((2,)),
            dma((n_fs,)),
            dma((n_fs, n_y - 1)),
            dma((3,)),
            dma((2,)),
            dma((2, n_y - 1, SHARE_CHUNKS)),
            dma((SHARE_CHUNKS,)),
            dma((3,)),
            dma((steps,)),
            dma((steps, n_y - 1)),
            dma((steps,)),
        ],
        compiler_params=pltpu.CompilerParams(
            collective_id=0, has_side_effects=True, vmem_limit_bytes=60 * 1024 * 1024
        ),
    )(
        tokens,
        gain1.reshape(1, -1),
        in_w,
        group_w,
        pool_scale.reshape(1, -1),
        out_w,
        gain2.reshape(1, -1),
        up_w,
        down_w,
    )


def solution(mesh):
    sizes = tuple(mesh.shape[axis] for axis in ("rep", "fs", "tp"))
    in_specs = (
        P(("rep", "fs", "tp"), None),
        P(),
        P("fs", "tp"),
        P("tp", None, None),
        P("tp"),
        P("tp", "fs"),
        P(),
        P("fs", "tp"),
        P("tp", "fs"),
    )
    return jax.shard_map(
        functools.partial(local, sizes),
        mesh=mesh,
        in_specs=in_specs,
        out_specs=P(("rep", "fs", "tp"), None),
        check_vma=False,
    )
```
